512 devices in a mesh: tp: 64 (over z, y), dp: 8 (over x, core).
Axes of the slice: x: 4, y: 8, z: 8, core: 2. Of those that a mesh axis runs over, the one named last changes fastest.
Arguments:
- tokens: bfloat16 [256, 4096], P(None, 'dp'), may hold values from -20 to 20
- norm_gain: float32 [2, 4096], P(None, 'dp'), may hold values from 0.1 to 1.9
- receptance: bfloat16 [2, 4096, 4096], P(None, 'dp', 'tp'), may hold values from -0.09375 to 0.09375
- key_proj: bfloat16 [2, 4096, 4096], P(None, 'dp', 'tp'), may hold values from -0.09375 to 0.09375
- value_proj: bfloat16 [2, 4096, 4096], P(None, 'dp', 'tp'), may hold values from -0.09375 to 0.09375
- decay_proj: bfloat16 [2, 4096, 4096], P(None, 'dp', 'tp'), may hold values from -0.09375 to 0.09375
- rate_proj: bfloat16 [2, 4096, 4096], P(None, 'dp', 'tp'), may hold values from -0.09375 to 0.09375
- gate_proj: bfloat16 [2, 4096, 4096], P(None, 'dp', 'tp'), may hold values from -0.09375 to 0.09375
- decay_base: float32 [2, 4096], P(None, 'tp'), may hold values from -6 to 1
- group_gain: float32 [2, 4096], P(None, 'tp'), may hold values from 0.1 to 1.9
- output_proj: bfloat16 [2, 4096, 4096], P(None, 'tp', 'dp'), may hold values from -0.09375 to 0.09375
- state: float32 [2, 256, 64, 4096], P(None, 'dp', 'tp'), may hold values from -3 to 3
Outputs:
- next_tokens: bfloat16 [256, 4096], P(None, 'dp')
- new_state: float32 [2, 256, 64, 4096], P(None, 'dp', 'tp')
The draws below stay inside these ranges and needn't reach their ends.
All inputs are finite; a program needn't handle non-finite values.
Results may differ from the reference program's by a relative error of at most 0.0066.
Values may be sent and summed in bfloat16 or wider, within the bound.
A program may use at most 64 MiB of HBM per device.

```python
import jax
import jax.numpy as jnp
from jax import lax

D = 4096
HEAD = 64
HEADS = 64
D_ATT = 4096
LAYERS = 2
BATCH = 256


def draw_tokens(key, part):
    base_key, row_key = jax.random.split(key)
    position = jnp.arange(D, dtype=jnp.float32) / D
    feature_scale = 0.4 + 1.6 * position
    row_scale = jnp.exp(jax.random.uniform(row_key, (BATCH, 1), jnp.float32, -0.6, 0.6))
    values = jnp.clip(jax.random.normal(base_key, (BATCH, D), jnp.float32), -5.0, 5.0)
    return (values * feature_scale[None, :] * row_scale).astype(jnp.bfloat16)


def block_levels(stream_key, shape, pieces, low, high):
    def one(axis_at, blocks):
        draws = jax.random.uniform(jax.random.fold_in(jax.random.fold_in(stream_key, 6), axis_at), (blocks,), jnp.float32, low / len(pieces), high / len(pieces))
        return jnp.repeat(jnp.exp(draws), shape[axis_at] // blocks).reshape((-1,) + (1,) * (len(shape) - axis_at - 1))

    level = one(*pieces[0])
    for cut in pieces[1:]:
        level = level * one(*cut)
    return level


def gaussian(stream_key, shape, deviation, limit, cuts=(), held_as=jnp.bfloat16):
    loudness = block_levels(stream_key, shape, cuts, -0.22, 0.18) if cuts else 1.0
    drawn = jax.random.normal(stream_key, shape, jnp.float32) * deviation * loudness
    return jnp.minimum(jnp.maximum(drawn, -limit), limit).astype(held_as)


def setup_inputs(seed: int = 0) -> dict:
    arg_keys = jax.random.split(jax.random.key(seed), 13)
    return {
        "tokens": draw_tokens(jax.random.fold_in(arg_keys[12], 71), 0),
        "norm_gain": jnp.clip(1.0 + 0.18 * jax.random.normal(arg_keys[1], (LAYERS, D), jnp.float32), 0.1, 1.9),
        "receptance": gaussian(arg_keys[2], (LAYERS, D, D_ATT), D ** -0.5, 0.09375, ((1, 8), (2, 64))),
        "key_proj": gaussian(arg_keys[3], (LAYERS, D, D_ATT), D ** -0.5, 0.09375, ((1, 8), (2, 64))),
        "value_proj": gaussian(arg_keys[4], (LAYERS, D, D_ATT), D ** -0.5, 0.09375, ((1, 8), (2, 64))),
        "decay_proj": gaussian(arg_keys[5], (LAYERS, D, D_ATT), D ** -0.5, 0.09375, ((1, 8), (2, 64))),
        "rate_proj": gaussian(arg_keys[6], (LAYERS, D, D_ATT), D ** -0.5, 0.09375, ((1, 8), (2, 64))),
        "gate_proj": gaussian(arg_keys[7], (LAYERS, D, D_ATT), D ** -0.5, 0.09375, ((1, 8), (2, 64))),
        "decay_base": jnp.clip(-6.0 + 7.0 * jax.random.uniform(arg_keys[8], (LAYERS, D_ATT), jnp.float32) ** block_levels(arg_keys[8], (LAYERS, D_ATT), ((1, 64),), -0.2, 0.2), -6.0, 1.0),
        "group_gain": jnp.clip(1.0 + 0.18 * jax.random.normal(arg_keys[9], (LAYERS, D_ATT), jnp.float32), 0.1, 1.9),
        "output_proj": gaussian(arg_keys[10], (LAYERS, D_ATT, D), D_ATT ** -0.5, 0.09375, ((1, 64), (2, 8))),
        "state": gaussian(arg_keys[11], (LAYERS, BATCH, HEADS, HEAD * HEAD), 0.5, 3.0, ((1, 8), (2, 64)), jnp.float32),
    }


norm_floor = 0.1
group_floor = 0.5

def recurrence(state_block, recept_heads, key_heads, value_heads, decay_heads, rate_heads):
    log_rate = -jax.nn.softplus(-decay_heads) - 0.5
    forget = jnp.exp(-jnp.exp(log_rate))
    learn_rate = jax.nn.sigmoid(rate_heads)
    unit_key = key_heads * lax.rsqrt(lax.optimization_barrier(jnp.sum(key_heads * key_heads, axis=-1, keepdims=True)) + 1.0)
    scaled = key_heads * learn_rate
    removed = jnp.einsum('bhvk,bhk->bhv', state_block, -unit_key, precision=lax.Precision.HIGHEST)
    updated = state_block * forget[:, :, None, :] + removed[..., None] * (unit_key * learn_rate)[:, :, None, :] + value_heads[..., None] * scaled[:, :, None, :]
    read_out = jnp.einsum('bhvk,bhk->bhv', updated, recept_heads, precision=lax.Precision.HIGHEST)
    centre = read_out - lax.optimization_barrier(jnp.mean(read_out, axis=-1, keepdims=True))
    normal = centre * lax.rsqrt(lax.optimization_barrier(jnp.mean(centre * centre, axis=-1, keepdims=True)) + group_floor)
    return (updated, normal)

def reference(tokens, norm_gain, receptance, key_proj, value_proj, decay_proj, rate_proj, gate_proj, decay_base, group_gain, output_proj, state):
    current = tokens
    finals = []
    for section_index in range(LAYERS):
        floats = current.astype(jnp.float32)
        squares = lax.optimization_barrier(jnp.sum(floats * floats, axis=1))
        inv_rms = lax.rsqrt(squares / D + norm_floor)
        normed = (floats * norm_gain[section_index]).astype(jnp.bfloat16)

        def by_head(weights):
            term = jnp.dot(normed, weights[section_index], preferred_element_type=jnp.float32)
            rounded = lax.optimization_barrier((inv_rms[:, None] * term).astype(jnp.bfloat16))
            return rounded.astype(jnp.float32).reshape(BATCH, HEADS, HEAD)
        decay_heads = by_head(decay_proj) + decay_base[section_index].reshape(1, HEADS, HEAD)
        updated, normal = recurrence(state[section_index].reshape(BATCH, HEADS, HEAD, HEAD), by_head(receptance), by_head(key_proj), by_head(value_proj), decay_heads, by_head(rate_proj))
        finals.append(updated.reshape(BATCH, HEADS, HEAD * HEAD))
        gate_value = jax.nn.sigmoid(by_head(gate_proj).reshape(BATCH, D_ATT))
        mixed_heads = (normal.reshape(BATCH, D_ATT) * group_gain[section_index] * gate_value).astype(jnp.bfloat16)
        branch = jnp.dot(mixed_heads, output_proj[section_index], preferred_element_type=jnp.float32)
        current = (floats + branch).astype(jnp.bfloat16)
    return (current, jnp.stack(finals))
```

```python
import jax
import jax.numpy as jnp
from jax import lax
from jax.experimental import pallas as pl
from jax.experimental.pallas import tpu as pltpu
from jax.sharding import PartitionSpec as P

D = 4096
HEAD = 64
LAYERS = 2
ROWS = 32
WIDE = 512
LANES = 128

norm_floor = 0.1
group_floor = 0.5

MESH = pl.DeviceIdType.MESH
RING8 = (4, 3, 5, 2, 6, 1, 7)
TP_OFFSETS = sorted(
    ((a, b) for a in range(8) for b in range(8) if (a, b) != (0, 0)),
    key=lambda ab: -(min(ab[0], 8 - ab[0]) + min(ab[1], 8 - ab[1])),
)


def iota(shape, dim):
    return lax.broadcasted_iota(jnp.int32, shape, dim)


def two_terms(x):
    high = x.astype(jnp.bfloat16)
    low = (x - high.astype(jnp.float32)).astype(jnp.bfloat16)
    return jnp.concatenate([high, low], axis=1)


def dot(a, b):
    return jnp.dot(a, b, preferred_element_type=jnp.float32)


def wait_for(ref, sem):
    pltpu.make_async_copy(ref, ref, sem).wait()


def body(
    tokens_ref,
    gain_ref,
    w0,
    w1,
    w2,
    w3,
    w4,
    w5,
    decay_ref,
    group_ref,
    out_proj_ref,
    state_ref,
    next_ref,
    new_state_ref,
    tokens,
    weights,
    wout,
    wdiag,
    state,
    part_send,
    part_recv,
    sq_send,
    sq_recv,
    mixed_all,
    out_send,
    out_recv,
    share,
    x_all,
    vec_g,
    vec_f,
    vec_s,
    vec_u,
    vec_v,
    read_rows,
    load_sem,
    late_sem,
    part_ssem,
    part_rsem,
    sq_ssem,
    sq_rsem,
    mix_ssem,
    mix_rsem,
    out_ssem,
    out_rsem,
    x_ssem,
    x_rsem,
    row_sem,
):
    tp = lax.axis_index("tp")
    dp = lax.axis_index("dp")
    z = tp // 8
    y = lax.rem(tp, 8)
    dp_peers = [(tp, lax.rem(dp + o, 8)) for o in RING8]
    y_peers = [(z * 8 + lax.rem(y + o, 8), dp) for o in RING8]
    z_peers = [(lax.rem(z + o, 8) * 8 + y, dp) for o in RING8]
    tp_peers = [(lax.rem(z + a, 8) * 8 + lax.rem(y + b, 8), dp) for a, b in TP_OFFSETS]

    barrier = pltpu.get_barrier_semaphore()
    for peer in dp_peers + y_peers + z_peers:
        pl.semaphore_signal(barrier, inc=1, device_id=peer, device_id_type=MESH)

    loads = [[], []]
    first = pltpu.make_async_copy(tokens_ref, tokens, load_sem.at[0])
    first.start()
    loads[0].append(first)
    for b in range(LAYERS):
        for n, w in enumerate((w0, w1, w2, w3, w4, w5)):
            copy = pltpu.make_async_copy(
                w.at[b], weights.at[b, pl.ds(n * HEAD, HEAD)], (load_sem if b == 0 else late_sem).at[n + 1]
            )
            copy.start()
            loads[b].append(copy)
        if b == 0:
            state_copy = pltpu.make_async_copy(state_ref, state, late_sem.at[0])
            state_copy.start()
            wout_copy = pltpu.make_async_copy(out_proj_ref, wout, load_sem.at[7])
            wout_copy.start()

    lane = iota((ROWS, LANES), 1)
    row = iota((ROWS, LANES), 0)
    low_half = lane < HEAD
    eye = (lane == row).astype(jnp.float32)
    pick = (lane % HEAD) // 2 == row
    pick_own = lane % HEAD == 2 * row + lane // HEAD
    ones = jnp.full((2 * LANES, LANES), 1.0, jnp.bfloat16)
    k_of = iota((2 * LANES, LANES), 0)
    l_of = iota((2 * LANES, LANES), 1)
    by_parity = ((k_of // HEAD) % 2 == l_of % 2).astype(jnp.float32).astype(jnp.bfloat16)
    by_half = ((k_of // HEAD) % 2 == l_of // HEAD).astype(jnp.float32).astype(jnp.bfloat16)

    sends = []

    def project(b, columns):
        squares = columns[0] * columns[0]
        for c in columns[1:]:
            squares = squares + c * c
        totals = dot(two_terms(squares), ones)
        for o in range(8):
            sq_send[b, o] = jnp.sum(totals[o * ROWS : (o + 1) * ROWS] * eye, axis=0, keepdims=True)
        normed = jnp.concatenate(
            [(c * gain_ref[b : b + 1, n * LANES : (n + 1) * LANES]).astype(jnp.bfloat16) for n, c in enumerate(columns)],
            axis=1,
        )
        for copy in loads[b][-6:]:
            copy.wait()
        part = lax.dot_general(
            normed, weights[b], (((1,), (1,)), ((), ())), preferred_element_type=jnp.float32
        ).astype(jnp.bfloat16)
        for o in range(8):
            part_send[b, o] = part[o * ROWS : (o + 1) * ROWS]

    def send_parts(b):
        for i, peer in enumerate(dp_peers):
            for src, dst, ssem, rsem in (
                (part_send, part_recv, part_ssem, part_rsem),
                (sq_send, sq_recv, sq_ssem, sq_rsem),
            ):
                pltpu.make_async_remote_copy(
                    src_ref=src.at[b, peer[1]],
                    dst_ref=dst.at[b, i],
                    send_sem=ssem.at[b],
                    recv_sem=rsem.at[b],
                    device_id=peer,
                    device_id_type=MESH,
                ).start()
        sends.append((part_recv.at[b], part_ssem.at[b]))
        sends.append((sq_recv.at[b], sq_ssem.at[b]))

    def mix(b):
        wait_for(sq_recv.at[b], sq_rsem.at[b])
        square = sq_send[b, dp]
        for i in range(7):
            square = square + sq_recv[b, i]
        inv = lax.rsqrt(jnp.sum(square * eye, axis=1, keepdims=True) / D + norm_floor)
        wait_for(part_recv.at[b], part_rsem.at[b])
        total = part_send[b, dp].astype(jnp.float32)
        for i in range(7):
            total = total + part_recv[b, i].astype(jnp.float32)
        heads = (total * inv).astype(jnp.bfloat16).astype(jnp.float32)
        both = []
        for n in range(3):
            tile = heads[:, n * LANES : (n + 1) * LANES]
            turned = pltpu.roll(tile, HEAD, 1)
            both.append(jnp.where(low_half, tile, turned))
            both.append(jnp.where(low_half, turned, tile))
        recept, keys, values, decay_in, rate_in, gate_in = both
        base = decay_ref[b : b + 1, :]
        decay = jnp.concatenate([base, base], axis=1) + decay_in
        forget = jnp.exp(-jnp.exp(-jax.nn.softplus(-decay) - 0.5))
        learn = jax.nn.sigmoid(rate_in)
        norm = lax.rsqrt(0.5 * jnp.sum(keys * keys, axis=1, keepdims=True) + 1.0)
        scaled = keys * learn
        with_scaled = 0.5 * jnp.sum(scaled * recept, axis=1, keepdims=True)
        unit = keys * norm
        vec_g[...] = forget * recept - (with_scaled * norm) * unit
        vec_f[...] = forget
        vec_s[...] = scaled
        vec_u[...] = unit * norm
        vec_v[...] = values
        for c in range(4):
            terms = jnp.concatenate(
                [state[b, r] * vec_g[r : r + 1, :] for r in range(c * 8, c * 8 + 8)], axis=0
            )
            sums = dot(two_terms(terms), by_parity)
            for r in range(8):
                at = c * 8 + r
                chosen = jnp.where(pick, sums[r * ROWS : (r + 1) * ROWS], 0.0)
                read_rows[at : at + 1, :] = jnp.sum(chosen, axis=0, keepdims=True)
        read = read_rows[...] + values * with_scaled
        centre = read - jnp.mean(read, axis=1, keepdims=True)
        normal = centre * lax.rsqrt(jnp.mean(centre * centre, axis=1, keepdims=True) + group_floor)
        gain = group_ref[b : b + 1, :]
        mixed = (normal * jnp.concatenate([gain, gain], axis=1) * jax.nn.sigmoid(gate_in)).astype(jnp.bfloat16)
        mixed_all[b, dp] = jnp.where(low_half[:16], mixed[:16], mixed[16:])

    def send_mixed(b):
        for peer in dp_peers:
            pltpu.make_async_remote_copy(
                src_ref=mixed_all.at[b, dp],
                dst_ref=mixed_all.at[b, dp],
                send_sem=mix_ssem.at[b],
                recv_sem=mix_rsem.at[b],
                device_id=peer,
                device_id_type=MESH,
            ).start()
        sends.append((mixed_all.at[b, pl.ds(0, 7)], mix_ssem.at[b]))

    def project_out(b):
        wait_for(mixed_all.at[b, pl.ds(0, 7)], mix_rsem.at[b])
        rows = mixed_all[b].reshape(8 * 16, LANES)
        for half in range(2):
            term = dot(rows, wdiag[b, half]).astype(jnp.bfloat16)
            for o in range(8):
                for c in range(4):
                    out_send[b, (o * 2 + half) * 4 + c] = term[o * 16 : (o + 1) * 16, c * LANES : (c + 1) * LANES]

    def send_out(b):
        for i, peer in enumerate(tp_peers):
            pltpu.make_async_remote_copy(
                src_ref=out_send.at[b, peer[0]],
                dst_ref=out_recv.at[b, i],
                send_sem=out_ssem.at[b],
                recv_sem=out_rsem.at[b],
                device_id=peer,
                device_id_type=MESH,
            ).start()
        sends.append((out_recv.at[b], out_ssem.at[b]))

    def update_state(b):
        for c in range(4):
            terms = jnp.concatenate(
                [
                    jnp.where(pick_own, vec_v[r : r + 1, :], 0.0) - state[b, r] * vec_u[r : r + 1, :]
                    for r in range(c * 8, c * 8 + 8)
                ],
                axis=0,
            )
            sums = dot(two_terms(terms), by_half)
            for r in range(8):
                at = c * 8 + r
                new_state_ref[b, at] = (
                    state[b, at] * vec_f[at : at + 1, :]
                    + sums[r * ROWS : (r + 1) * ROWS] * vec_s[at : at + 1, :]
                )

    def finish_share(b, mine):
        wait_for(out_recv.at[b], out_rsem.at[b])
        parts = [out_send[b, tp].astype(jnp.float32)] + [jnp.zeros((16, LANES), jnp.float32)] * 3
        for i in range(63):
            parts[(i + 1) % 4] = parts[(i + 1) % 4] + out_recv[b, i].astype(jnp.float32)
        total = (parts[0] + parts[1]) + (parts[2] + parts[3])
        new = (mine.astype(jnp.float32) + total).astype(jnp.bfloat16)
        share[b] = new
        x_all[b, tp] = new

    def send_share(b):
        for peer in tp_peers:
            pltpu.make_async_remote_copy(
                src_ref=share.at[b],
                dst_ref=x_all.at[b, tp],
                send_sem=x_ssem.at[b],
                recv_sem=x_rsem.at[b],
                device_id=peer,
                device_id_type=MESH,
            ).start()
        sends.append((x_all.at[b, pl.ds(0, 63)], x_ssem.at[b]))

    first.wait()
    project(0, [tokens[:, c * LANES : (c + 1) * LANES].astype(jnp.float32) for c in range(4)])
    pl.semaphore_wait(barrier, 21)
    send_parts(0)
    for peer in z_peers:
        pl.semaphore_signal(row_sem, inc=1, device_id=peer, device_id_type=MESH)
    wout_copy.wait()
    wdiag[...] = jnp.zeros_like(wdiag)
    for b in range(LAYERS):
        wdiag[b, 0, 0:HEAD] = wout[b]
        wdiag[b, 1, HEAD : 2 * HEAD] = wout[b]
    state_copy.wait()
    mix(0)
    send_mixed(0)
    pl.semaphore_wait(row_sem, 7)
    project_out(0)
    send_out(0)
    update_state(0)
    at_row = pl.multiple_of((tp // 4) * 16, 16)
    at_column = pl.multiple_of(lax.rem(tp, 4) * LANES, LANES)
    finish_share(0, tokens[pl.ds(at_row, 16), pl.ds(at_column, LANES)])
    send_share(0)
    wait_for(x_all.at[0, pl.ds(0, 63)], x_rsem.at[0])

    columns = [
        jnp.concatenate([x_all[0, g * 4 + c].astype(jnp.float32) for g in range(16)], axis=0) for c in range(4)
    ]
    project(1, columns)
    send_parts(1)
    mix(1)
    send_mixed(1)
    project_out(1)
    send_out(1)
    update_state(1)
    finish_share(1, share[0])
    send_share(1)
    wait_for(x_all.at[1, pl.ds(0, 63)], x_rsem.at[1])
    for g in range(16):
        for c in range(4):
            next_ref[g * 16 : (g + 1) * 16, c * LANES : (c + 1) * LANES] = x_all[1, g * 4 + c]
    for ref, sem in sends:
        wait_for(ref, sem)


def shards(
    tokens,
    norm_gain,
    receptance,
    key_proj,
    value_proj,
    decay_proj,
    rate_proj,
    gate_proj,
    decay_base,
    group_gain,
    output_proj,
    state,
):
    flat = [jnp.swapaxes(w, 1, 2) for w in (receptance, key_proj, value_proj, decay_proj, rate_proj, gate_proj)]
    remote = pl.BlockSpec(memory_space=pltpu.HBM)
    local = pl.BlockSpec(memory_space=pltpu.VMEM)
    f32, bf16 = jnp.float32, jnp.bfloat16
    dma = pltpu.SemaphoreType.DMA
    current, updated = pl.pallas_call(
        body,
        out_shape=(
            jax.ShapeDtypeStruct((256, WIDE), bf16),
            jax.ShapeDtypeStruct((LAYERS, ROWS, 32, LANES), f32),
        ),
        in_specs=[remote, local] + [remote] * 6 + [local, local, remote, remote],
        out_specs=(local, local),
        scratch_shapes=[
            pltpu.VMEM((256, WIDE), bf16),
            pltpu.VMEM((LAYERS, 6 * HEAD, WIDE), bf16),
            pltpu.VMEM((LAYERS, HEAD, WIDE), bf16),
            pltpu.VMEM((LAYERS, 2, LANES, WIDE), bf16),
            pltpu.VMEM((LAYERS, ROWS, 32, LANES), f32),
            pltpu.VMEM((LAYERS, 8, ROWS, 6 * HEAD), bf16),
            pltpu.VMEM((LAYERS, 7, ROWS, 6 * HEAD), bf16),
            pltpu.VMEM((LAYERS, 8, 1, LANES), f32),
            pltpu.VMEM((LAYERS, 7, 1, LANES), f32),
            pltpu.VMEM((LAYERS, 8, 16, LANES), bf16),
            pltpu.VMEM((LAYERS, 64, 16, LANES), bf16),
            pltpu.VMEM((LAYERS, 63, 16, LANES), bf16),
            pltpu.VMEM((LAYERS, 16, LANES), bf16),
            pltpu.VMEM((LAYERS, 64, 16, LANES), bf16),
        ]
        + [pltpu.VMEM((ROWS, LANES), f32)] * 6
        + [dma((8,)), dma((7,))]
        + [dma((LAYERS,))] * 10
        + [pltpu.SemaphoreType.REGULAR],
        compiler_params=pltpu.CompilerParams(
            collective_id=0, has_side_effects=True, vmem_limit_bytes=67043328
        ),
        name="blocks",
    )(tokens, norm_gain, *flat, decay_base, group_gain, output_proj, state.reshape(LAYERS, ROWS, 32, LANES))
    return (current, updated.reshape(LAYERS, ROWS, 1, HEAD * HEAD))


def solution(mesh):
    return jax.shard_map(
        shards,
        mesh=mesh,
        in_specs=(
            P(None, "dp"),
            P(None, "dp"),
            P(None, "dp", "tp"),
            P(None, "dp", "tp"),
            P(None, "dp", "tp"),
            P(None, "dp", "tp"),
            P(None, "dp", "tp"),
            P(None, "dp", "tp"),
            P(None, "tp"),
            P(None, "tp"),
            P(None, "tp", "dp"),
            P(None, "dp", "tp", None),
        ),
        out_specs=(P(None, "dp"), P(None, "dp", "tp", None)),
        check_vma=False,
    )
```

```python
import jax
import jax.numpy as jnp
from jax import lax
from jax.experimental import pallas as pl
from jax.experimental.pallas import tpu as pltpu
from jax.sharding import PartitionSpec as P

D = 4096
HEAD = 64
LAYERS = 2
ROWS = 32
WIDE = 512
LANES = 128

norm_floor = 0.1
group_floor = 0.5

MESH = pl.DeviceIdType.MESH
RING8 = (4, 3, 5, 2, 6, 1, 7)
TP_OFFSETS = sorted(
    ((a, b) for a in range(8) for b in range(8) if (a, b) != (0, 0)),
    key=lambda ab: -(min(ab[0], 8 - ab[0]) + min(ab[1], 8 - ab[1])),
)


def iota(shape, dim):
    return lax.broadcasted_iota(jnp.int32, shape, dim)


def two_terms(x):
    high = x.astype(jnp.bfloat16)
    low = (x - high.astype(jnp.float32)).astype(jnp.bfloat16)
    return jnp.concatenate([high, low], axis=1)


def dot(a, b):
    return jnp.dot(a, b, preferred_element_type=jnp.float32)


def wait_for(ref, sem):
    pltpu.make_async_copy(ref, ref, sem).wait()


def body(
    tokens_ref,
    gain_in,
    w0,
    w1,
    w2,
    w3,
    w4,
    w5,
    decay_in,
    group_in,
    out_proj_ref,
    state_ref,
    next_ref,
    new_state_ref,
    tokens,
    first_weights,
    weights,
    wout,
    gains,
    decay_ref,
    group_ref,
    residue,
    state,
    part_send,
    part_recv,
    sq_send,
    sq_recv,
    out_send,
    out_recv,
    share,
    x_all,
    x_last,
    vec_g,
    vec_f,
    vec_s,
    vec_u,
    vec_v,
    read_rows,
    load_sem,
    late_sem,
    part_sem,
    sq_sem,
    out_sem,
    x_sem,
    gain_sem,
    residue_sem,
    wout_sem,
    wout_core_sem,
    ring_sem,
    core_sem,
    last_sem,
    row_sem,
    plane_sem,
):
    tp = lax.axis_index("tp")
    dp = lax.axis_index("dp")
    z = tp // 8
    y = lax.rem(tp, 8)
    x = dp // 2
    core = lax.rem(dp, 2)
    dp_peers = [(tp, lax.rem(dp + o, 8)) for o in RING8]
    y_peers = [(z * 8 + lax.rem(y + o, 8), dp) for o in RING8]
    z_peers = [(lax.rem(z + o, 8) * 8 + y, dp) for o in RING8]
    tp_peers = [(lax.rem(z + a, 8) * 8 + lax.rem(y + b, 8), dp) for a, b in TP_OFFSETS]
    right, far, left = (lax.rem(x + o, 4) * 2 + core for o in (1, 2, 3))
    partner = x * 2 + (1 - core)
    owns_columns = dp == z
    half_row = lax.rem(y, 2)
    column = y // 2

    def remote(src, dst, sems, peer):
        copy = pltpu.make_async_remote_copy(
            src_ref=src, dst_ref=dst, send_sem=sems[0], recv_sem=sems[1], device_id=peer, device_id_type=MESH
        )
        copy.start()
        return copy

    barrier = pltpu.get_barrier_semaphore()
    for peer in dp_peers + y_peers + z_peers:
        pl.semaphore_signal(barrier, inc=1, device_id=peer, device_id_type=MESH)

    def load(src, dst, sem):
        copy = pltpu.make_async_copy(src, dst, sem)
        copy.start()
        return copy

    tokens_load = load(tokens_ref, tokens, load_sem.at[0])
    gain_load = load(gain_in, gains.at[dp], load_sem.at[7])
    small_loads = [load(decay_in, decay_ref, load_sem.at[8]), load(group_in, group_ref, load_sem.at[9])]
    projections = (w0, w1, w2, w3, w4, w5)
    first_loads = [
        load(w.at[0], first_weights.at[pl.ds(n * HEAD, HEAD)], load_sem.at[n + 1]) for n, w in enumerate(projections)
    ]
    wout_loads = [load(out_proj_ref.at[b], wout.at[b, dp], late_sem.at[7 + b]) for b in range(LAYERS)]
    state_load = load(state_ref, state, late_sem.at[0])
    weight_loads = [
        load(w.at[1], weights.at[dp, pl.ds(n * HEAD, HEAD)], late_sem.at[n + 1]) for n, w in enumerate(projections)
    ]

    lane = iota((ROWS, LANES), 1)
    row = iota((ROWS, LANES), 0)
    low_half = lane < HEAD
    eye = (lane == row).astype(jnp.float32)
    pick = (lane % HEAD) // 2 == row
    pick_own = lane % HEAD == 2 * row + lane // HEAD
    ones = jnp.full((2 * LANES, LANES), 1.0, jnp.bfloat16)
    k_of = iota((2 * LANES, LANES), 0)
    l_of = iota((2 * LANES, LANES), 1)
    by_parity = ((k_of // HEAD) % 2 == l_of % 2).astype(jnp.float32).astype(jnp.bfloat16)
    by_half = ((k_of // HEAD) % 2 == l_of // HEAD).astype(jnp.float32).astype(jnp.bfloat16)

    waits = []

    def first_parts():
        columns = [tokens[:, c * LANES : (c + 1) * LANES].astype(jnp.float32) for c in range(4)]
        squares = columns[0] * columns[0]
        for c in columns[1:]:
            squares = squares + c * c
        totals = dot(two_terms(squares), ones)
        for o in range(8):
            sq_send[o] = jnp.sum(totals[o * ROWS : (o + 1) * ROWS] * eye, axis=0, keepdims=True)
        gain_load.wait()
        normed = jnp.concatenate(
            [(c * gains[dp, 0:1, n * LANES : (n + 1) * LANES]).astype(jnp.bfloat16) for n, c in enumerate(columns)],
            axis=1,
        )
        for copy in first_loads:
            copy.wait()
        part = lax.dot_general(
            normed, first_weights[...], (((1,), (1,)), ((), ())), preferred_element_type=jnp.float32
        ).astype(jnp.bfloat16)
        for o in range(8):
            part_send[o] = part[o * ROWS : (o + 1) * ROWS]

    def send_parts():
        for i, peer in enumerate(dp_peers):
            remote(part_send.at[peer[1]], part_recv.at[i], (part_sem.at[0], part_sem.at[1]), peer)
            remote(sq_send.at[peer[1]], sq_recv.at[i], (sq_sem.at[0], sq_sem.at[1]), peer)
        waits.append((part_recv, part_sem.at[0]))
        waits.append((sq_recv, sq_sem.at[0]))

    def first_projected():
        wait_for(sq_recv, sq_sem.at[1])
        square = sq_send[dp]
        for i in range(7):
            square = square + sq_recv[i]
        inv = lax.rsqrt(jnp.sum(square * eye, axis=1, keepdims=True) / D + norm_floor)
        wait_for(part_recv, part_sem.at[1])
        total = part_send[dp].astype(jnp.float32)
        for i in range(7):
            total = total + part_recv[i].astype(jnp.float32)
        return total * inv

    def second_projected():
        squares = jnp.zeros((ROWS, LANES), jnp.float32)
        total = jnp.zeros((ROWS, 6 * HEAD), jnp.float32)
        for d in range(8):
            pieces = []
            for c in range(4):
                at = (d * 4 + c) * 2
                piece = jnp.concatenate([x_all[at], x_all[at + 1]], axis=0).astype(jnp.float32)
                squares = squares + piece * piece
                pieces.append((piece * gains[d, 1:2, c * LANES : (c + 1) * LANES]).astype(jnp.bfloat16))
            total = total + lax.dot_general(
                jnp.concatenate(pieces, axis=1),
                weights[d],
                (((1,), (1,)), ((), ())),
                preferred_element_type=jnp.float32,
            )
        inv = lax.rsqrt(jnp.sum(squares, axis=1, keepdims=True) / D + norm_floor)
        return total * inv

    def mix(b, projected):
        heads = projected.astype(jnp.bfloat16).astype(jnp.float32)
        both = []
        for n in range(3):
            tile = heads[:, n * LANES : (n + 1) * LANES]
            turned = pltpu.roll(tile, HEAD, 1)
            both.append(jnp.where(low_half, tile, turned))
            both.append(jnp.where(low_half, turned, tile))
        recept, keys, values, decay_part, rate_part, gate_part = both
        base = decay_ref[b : b + 1, :]
        decay = jnp.concatenate([base, base], axis=1) + decay_part
        forget = jnp.exp(-jnp.exp(-jax.nn.softplus(-decay) - 0.5))
        learn = jax.nn.sigmoid(rate_part)
        norm = lax.rsqrt(0.5 * jnp.sum(keys * keys, axis=1, keepdims=True) + 1.0)
        scaled = keys * learn
        with_scaled = 0.5 * jnp.sum(scaled * recept, axis=1, keepdims=True)
        unit = keys * norm
        vec_g[...] = forget * recept - (with_scaled * norm) * unit
        vec_f[...] = forget
        vec_s[...] = scaled
        vec_u[...] = unit * norm
        vec_v[...] = values
        for c in range(4):
            terms = jnp.concatenate([state[b, r] * vec_g[r : r + 1, :] for r in range(c * 8, c * 8 + 8)], axis=0)
            sums = dot(two_terms(terms), by_parity)
            for r in range(8):
                at = c * 8 + r
                chosen = jnp.where(pick, sums[r * ROWS : (r + 1) * ROWS], 0.0)
                read_rows[at : at + 1, :] = jnp.sum(chosen, axis=0, keepdims=True)
        read = read_rows[...] + values * with_scaled
        centre = read - jnp.mean(read, axis=1, keepdims=True)
        normal = centre * lax.rsqrt(jnp.mean(centre * centre, axis=1, keepdims=True) + group_floor)
        gain = group_ref[b : b + 1, :]
        return (normal * jnp.concatenate([gain, gain], axis=1) * jax.nn.sigmoid(gate_part)).astype(jnp.bfloat16)

    def project_out(b, mixed):
        rows = mixed[:, :HEAD]
        for d in range(8):
            term = dot(rows, wout[b, d]).astype(jnp.bfloat16)
            for c in range(4):
                for half in range(2):
                    out_send[b, (d * 4 + c) * 2 + half] = term[
                        half * 16 : (half + 1) * 16, c * LANES : (c + 1) * LANES
                    ]

    def send_out(b):
        for i, peer in enumerate(tp_peers):
            remote(out_send.at[b, peer[0]], out_recv.at[b, i], (out_sem.at[b], out_sem.at[2 + b]), peer)
        waits.append((out_recv.at[b], out_sem.at[b]))

    def update_state(b):
        for c in range(4):
            terms = jnp.concatenate(
                [
                    jnp.where(pick_own, vec_v[r : r + 1, :], 0.0) - state[b, r] * vec_u[r : r + 1, :]
                    for r in range(c * 8, c * 8 + 8)
                ],
                axis=0,
            )
            sums = dot(two_terms(terms), by_half)
            for r in range(8):
                at = c * 8 + r
                new_state_ref[b, at] = (
                    state[b, at] * vec_f[at : at + 1, :] + sums[r * ROWS : (r + 1) * ROWS] * vec_s[at : at + 1, :]
                )

    def finish_share(b, mine):
        wait_for(out_recv.at[b], out_sem.at[2 + b])
        parts = [out_send[b, tp].astype(jnp.float32)] + [jnp.zeros((16, LANES), jnp.float32)] * 3
        for i in range(63):
            parts[(i + 1) % 4] = parts[(i + 1) % 4] + out_recv[b, i].astype(jnp.float32)
        total = (parts[0] + parts[1]) + (parts[2] + parts[3])
        share[b] = (mine.astype(jnp.float32) + total).astype(jnp.bfloat16)

    def gather_wout(b):
        wout_loads[b].wait()
        for peer in (far, right, left):
            remote(wout.at[b, dp], wout.at[b, dp], (wout_sem.at[b], wout_sem.at[2 + b]), (tp, peer))
        remote(wout.at[b, dp], wout.at[b, dp], (wout_core_sem.at[b], wout_core_sem.at[2 + b]), (tp, partner))
        waits.append((wout.at[b, pl.ds(0, 3)], wout_sem.at[b]))

    def pass_wout(b):
        wait_for(wout.at[b, pl.ds(0, 3)], wout_sem.at[2 + b])
        for peer in (far, right, left):
            remote(
                wout.at[b, peer], wout.at[b, peer], (wout_core_sem.at[b], wout_core_sem.at[2 + b]), (tp, partner)
            )
        waits.append((wout.at[b, pl.ds(0, 4)], wout_core_sem.at[b]))

    half_rows = 3 * HEAD

    def gather_weights():
        for copy in weight_loads:
            copy.wait()
        mine = weights.at[dp]
        remote(mine, mine, (ring_sem.at[0], ring_sem.at[4]), (tp, right))
        remote(mine, mine, (ring_sem.at[1], ring_sem.at[5]), (tp, left))
        remote(mine, mine, (core_sem.at[0], core_sem.at[1]), (tp, partner))
        waits.append((mine, ring_sem.at[0]))
        waits.append((mine, ring_sem.at[1]))

    def pass_weights():
        first, second = pl.ds(0, half_rows), pl.ds(half_rows, half_rows)
        from_left, from_right = weights.at[left], weights.at[right]
        wait_for(from_left, ring_sem.at[4])
        remote(weights.at[left, first], weights.at[left, first], (ring_sem.at[2], ring_sem.at[6]), (tp, right))
        wait_for(from_right, ring_sem.at[5])
        remote(weights.at[right, second], weights.at[right, second], (ring_sem.at[3], ring_sem.at[7]), (tp, left))
        remote(from_left, from_left, (core_sem.at[0], core_sem.at[1]), (tp, partner))
        remote(from_right, from_right, (core_sem.at[0], core_sem.at[1]), (tp, partner))
        waits.append((weights.at[left, first], ring_sem.at[2]))
        waits.append((weights.at[left, first], ring_sem.at[3]))

    def end_weights():
        wait_for(weights.at[far, pl.ds(0, half_rows)], ring_sem.at[6])
        wait_for(weights.at[far, pl.ds(0, half_rows)], ring_sem.at[7])
        remote(weights.at[far], weights.at[far], (core_sem.at[0], core_sem.at[1]), (tp, partner))
        waits.append((weights.at[pl.ds(0, 4)], core_sem.at[0]))
        wait_for(weights.at[pl.ds(0, 4)], core_sem.at[1])

    tokens_load.wait()
    first_parts()
    pl.semaphore_wait(barrier, 21)
    send_parts()
    gather_wout(0)
    for peer in dp_peers:
        remote(gains.at[dp], gains.at[dp], (gain_sem.at[0], gain_sem.at[1]), peer)
    waits.append((gains.at[pl.ds(0, 7)], gain_sem.at[0]))
    at_column = pl.ds(pl.multiple_of(column * LANES, LANES), LANES)

    def at_rows(owner):
        return pl.ds(pl.multiple_of(owner * ROWS + half_row * 16, 16), 16)

    @pl.when(owns_columns)
    def _():
        for peer in dp_peers:
            remote(tokens.at[at_rows(peer[1]), at_column], residue, (residue_sem.at[0], residue_sem.at[1]), peer)
        residue[...] = tokens[at_rows(dp), at_column]

    for peer in z_peers:
        pl.semaphore_signal(row_sem, inc=1, device_id=peer, device_id_type=MESH)
    gather_weights()
    pass_wout(0)
    projected = first_projected()
    for copy in small_loads + [state_load]:
        copy.wait()
    mixed = mix(0, projected)
    pl.semaphore_wait(row_sem, 7)
    for peer in dp_peers:
        pl.semaphore_signal(plane_sem, inc=1, device_id=peer, device_id_type=MESH)
    wait_for(wout.at[0, pl.ds(0, 4)], wout_core_sem.at[2])
    project_out(0, mixed)
    send_out(0)
    update_state(0)

    @pl.when(jnp.logical_not(owns_columns))
    def _():
        wait_for(residue, residue_sem.at[1])

    finish_share(0, residue[...])
    x_all[tp] = share[0]
    for peer in tp_peers:
        remote(share.at[0], x_all.at[tp], (x_sem.at[0], x_sem.at[1]), peer)
    waits.append((x_all.at[pl.ds(0, 63)], x_sem.at[0]))
    pass_weights()
    gather_wout(1)
    pass_wout(1)
    wait_for(gains.at[pl.ds(0, 7)], gain_sem.at[1])
    pl.semaphore_wait(plane_sem, 7)
    end_weights()
    wait_for(wout.at[1, pl.ds(0, 4)], wout_core_sem.at[3])
    wait_for(x_all.at[pl.ds(0, 63)], x_sem.at[1])

    project_out(1, mix(1, second_projected()))
    send_out(1)
    update_state(1)
    finish_share(1, share[0])
    slot = (dp * 2 + half_row) * 4 + column

    @pl.when(jnp.logical_not(owns_columns))
    def _():
        remote(share.at[1], x_last.at[slot], (last_sem.at[2], last_sem.at[1]), (tp, z))

    @pl.when(owns_columns)
    def _():
        load(share.at[1], x_last.at[slot], last_sem.at[1])

    for peer in tp_peers:
        remote(share.at[1], x_last.at[slot], (last_sem.at[0], last_sem.at[1]), (peer[0], z))
    waits.append((x_last.at[pl.ds(0, 63)], last_sem.at[0]))
    wait_for(x_last, last_sem.at[1])
    for g in range(16):
        for c in range(4):
            next_ref[g * 16 : (g + 1) * 16, c * LANES : (c + 1) * LANES] = x_last[g * 4 + c]

    @pl.when(jnp.logical_not(owns_columns))
    def _():
        wait_for(share.at[1], last_sem.at[2])

    @pl.when(owns_columns)
    def _():
        wait_for(x_last.at[pl.ds(0, 7)], residue_sem.at[0])

    for ref, sem in waits:
        wait_for(ref, sem)


def write_out(next_ref, state_ref, next_out, state_out, sems):
    copies = [
        pltpu.make_async_copy(src, dst, sems.at[n])
        for n, (src, dst) in enumerate(((state_ref, state_out), (next_ref, next_out)))
    ]
    for copy in copies:
        copy.start()
    for copy in copies:
        copy.wait()


def shards(
    tokens,
    norm_gain,
    receptance,
    key_proj,
    value_proj,
    decay_proj,
    rate_proj,
    gate_proj,
    decay_base,
    group_gain,
    output_proj,
    state,
):
    flat = [jnp.swapaxes(w, 1, 2) for w in (receptance, key_proj, value_proj, decay_proj, rate_proj, gate_proj)]
    remote = pl.BlockSpec(memory_space=pltpu.HBM)
    local = pl.BlockSpec(memory_space=pltpu.VMEM)
    f32, bf16 = jnp.float32, jnp.bfloat16
    dma = pltpu.SemaphoreType.DMA

    current, updated = pl.pallas_call(
        body,
        out_shape=(
            pltpu.VMEM((256, WIDE), bf16),
            pltpu.VMEM((LAYERS, ROWS, 32, LANES), f32),
        ),
        in_specs=[remote] * 12,
        out_specs=(local, local),
        scratch_shapes=[
            pltpu.VMEM((256, WIDE), bf16),
            pltpu.VMEM((6 * HEAD, WIDE), bf16),
            pltpu.VMEM((8, 6 * HEAD, WIDE), bf16),
            pltpu.VMEM((LAYERS, 8, HEAD, WIDE), bf16),
            pltpu.VMEM((8, LAYERS, WIDE), f32),
            pltpu.VMEM((LAYERS, HEAD), f32),
            pltpu.VMEM((LAYERS, HEAD), f32),
            pltpu.VMEM((16, LANES), bf16),
            pltpu.VMEM((LAYERS, ROWS, 32, LANES), f32),
            pltpu.VMEM((8, ROWS, 6 * HEAD), bf16),
            pltpu.VMEM((7, ROWS, 6 * HEAD), bf16),
            pltpu.VMEM((8, 1, LANES), f32),
            pltpu.VMEM((7, 1, LANES), f32),
            pltpu.VMEM((LAYERS, 64, 16, LANES), bf16),
            pltpu.VMEM((LAYERS, 63, 16, LANES), bf16),
            pltpu.VMEM((LAYERS, 16, LANES), bf16),
            pltpu.VMEM((64, 16, LANES), bf16),
            pltpu.VMEM((64, 16, LANES), bf16),
        ]
        + [pltpu.VMEM((ROWS, LANES), f32)] * 6
        + [dma((10,)), dma((9,)), dma((2,)), dma((2,)), dma((4,)), dma((2,)), dma((2,)), dma((2,))]
        + [dma((4,)), dma((4,)), dma((8,)), dma((2,)), dma((3,))]
        + [pltpu.SemaphoreType.REGULAR] * 2,
        compiler_params=pltpu.CompilerParams(
            collective_id=0, has_side_effects=True, vmem_limit_bytes=32 * 1024 * 1024
        ),
        name="blocks",
    )(
        *[
            pltpu.with_memory_space_constraint(a, pltpu.HBM)
            for a in (
                tokens,
                norm_gain,
                *flat,
                decay_base,
                group_gain,
                output_proj,
                state.reshape(LAYERS, ROWS, 32, LANES),
            )
        ]
    )
    current, updated = pl.pallas_call(
        write_out,
        out_shape=(
            jax.ShapeDtypeStruct((256, WIDE), bf16),
            jax.ShapeDtypeStruct((LAYERS, ROWS, 32, LANES), f32),
        ),
        in_specs=[local, local],
        out_specs=(remote, remote),
        scratch_shapes=[dma((2,))],
        name="write_out",
    )(*[pltpu.with_memory_space_constraint(a, pltpu.VMEM) for a in (current, updated)])
    return (current, updated.reshape(LAYERS, ROWS, 1, HEAD * HEAD))


def solution(mesh):
    return jax.shard_map(
        shards,
        mesh=mesh,
        in_specs=(
            P(None, "dp"),
            P(None, "dp"),
            P(None, "dp", "tp"),
            P(None, "dp", "tp"),
            P(None, "dp", "tp"),
            P(None, "dp", "tp"),
            P(None, "dp", "tp"),
            P(None, "dp", "tp"),
            P(None, "tp"),
            P(None, "tp"),
            P(None, "tp", "dp"),
            P(None, "dp", "tp", None),
        ),
        out_specs=(P(None, "dp"), P(None, "dp", "tp", None)),
        check_vma=False,
    )
```

```python
import jax
import jax.numpy as jnp
from jax import lax
from jax.experimental import pallas as pl
from jax.experimental.pallas import tpu as pltpu
from jax.sharding import PartitionSpec as P

D = 4096
HEAD = 64
LAYERS = 2
ROWS = 32
WIDE = 512
LANES = 128

norm_floor = 0.1
group_floor = 0.5

MESH = pl.DeviceIdType.MESH
RING8 = (4, 3, 5, 2, 6, 1, 7)
TP_OFFSETS = sorted(
    ((a, b) for a in range(8) for b in range(8) if (a, b) != (0, 0)),
    key=lambda ab: -(min(ab[0], 8 - ab[0]) + min(ab[1], 8 - ab[1])),
)


def iota(shape, dim):
    return lax.broadcasted_iota(jnp.int32, shape, dim)


def two_terms(x):
    high = x.astype(jnp.bfloat16)
    low = (x - high.astype(jnp.float32)).astype(jnp.bfloat16)
    return jnp.concatenate([high, low], axis=1)


def dot(a, b):
    return jnp.dot(a, b, preferred_element_type=jnp.float32)


def wait_for(ref, sem):
    pltpu.make_async_copy(ref, ref, sem).wait()


def body(
    tokens_ref,
    gain_in,
    w0,
    w1,
    w2,
    w3,
    w4,
    w5,
    decay_in,
    group_in,
    out_proj_ref,
    state_ref,
    next_ref,
    new_state_ref,
    tokens,
    first_weights,
    weights,
    wout,
    gains,
    decay_ref,
    group_ref,
    residue,
    state,
    part_send,
    part_core,
    part_sum,
    part_recv,
    sq_send,
    sq_recv,
    out_send,
    out_recv,
    share,
    x_all,
    x_last,
    vec_g,
    vec_f,
    vec_s,
    vec_u,
    vec_v,
    read_rows,
    load_sem,
    late_sem,
    pair_sem,
    part_sem,
    sq_sem,
    out_sem,
    x_sem,
    gain_sem,
    residue_sem,
    wout_sem,
    wout_core_sem,
    ring_sem,
    core_sem,
    last_sem,
    near_sem,
    line_sem,
    row_sem,
    plane_sem,
):
    tp = lax.axis_index("tp")
    dp = lax.axis_index("dp")
    z = tp // 8
    y = lax.rem(tp, 8)
    x = dp // 2
    core = lax.rem(dp, 2)
    dp_peers = [(tp, lax.rem(dp + o, 8)) for o in RING8]
    z_peers = [(lax.rem(z + o, 8) * 8 + y, dp) for o in RING8]
    tp_peers = [(lax.rem(z + a, 8) * 8 + lax.rem(y + b, 8), dp) for a, b in TP_OFFSETS]
    right, far, left = (lax.rem(x + o, 4) * 2 + core for o in (1, 2, 3))
    partner = x * 2 + (1 - core)
    owns_columns = dp == z
    half_row = lax.rem(y, 2)
    column = y // 2

    def remote(src, dst, sems, peer):
        copy = pltpu.make_async_remote_copy(
            src_ref=src, dst_ref=dst, send_sem=sems[0], recv_sem=sems[1], device_id=peer, device_id_type=MESH
        )
        copy.start()
        return copy

    def beside(o):
        return [(z * 8 + lax.rem(y + k, 8), dp) for k in (o, 8 - o)] + [
            (lax.rem(z + k, 8) * 8 + y, dp) for k in (o, 8 - o)
        ]

    def tell(sem, peers):
        for peer in peers:
            pl.semaphore_signal(sem, inc=1, device_id=peer, device_id_type=MESH)

    barrier = pltpu.get_barrier_semaphore()
    tell(barrier, dp_peers + beside(1))

    def load(src, dst, sem):
        copy = pltpu.make_async_copy(src, dst, sem)
        copy.start()
        return copy

    tokens_load = load(tokens_ref, tokens, load_sem.at[0])
    gain_load = load(gain_in, gains.at[dp], load_sem.at[7])
    small_loads = [load(decay_in, decay_ref, load_sem.at[8]), load(group_in, group_ref, load_sem.at[9])]
    projections = (w0, w1, w2, w3, w4, w5)
    first_loads = [
        load(w.at[0], first_weights.at[pl.ds(n * HEAD, HEAD)], load_sem.at[n + 1]) for n, w in enumerate(projections)
    ]
    wout_loads = [load(out_proj_ref.at[b], wout.at[b, dp], late_sem.at[7 + b]) for b in range(LAYERS)]
    state_load = load(state_ref, state, late_sem.at[0])
    weight_loads = [
        load(w.at[1], weights.at[dp, pl.ds(n * HEAD, HEAD)], late_sem.at[n + 1]) for n, w in enumerate(projections)
    ]

    lane = iota((ROWS, LANES), 1)
    row = iota((ROWS, LANES), 0)
    low_half = lane < HEAD
    eye = (lane == row).astype(jnp.float32)
    pick = (lane % HEAD) // 2 == row
    pick_own = lane % HEAD == 2 * row + lane // HEAD
    ones = jnp.full((2 * LANES, LANES), 1.0, jnp.bfloat16)
    k_of = iota((2 * LANES, LANES), 0)
    l_of = iota((2 * LANES, LANES), 1)
    by_parity = ((k_of // HEAD) % 2 == l_of % 2).astype(jnp.float32).astype(jnp.bfloat16)
    by_half = ((k_of // HEAD) % 2 == l_of // HEAD).astype(jnp.float32).astype(jnp.bfloat16)

    waits = []

    def first_parts():
        columns = [tokens[:, c * LANES : (c + 1) * LANES].astype(jnp.float32) for c in range(4)]
        squares = columns[0] * columns[0]
        for c in columns[1:]:
            squares = squares + c * c
        totals = dot(two_terms(squares), ones)
        for o in range(8):
            sq_send[o] = jnp.sum(totals[o * ROWS : (o + 1) * ROWS] * eye, axis=0, keepdims=True)
        gain_load.wait()
        normed = jnp.concatenate(
            [(c * gains[dp, 0:1, n * LANES : (n + 1) * LANES]).astype(jnp.bfloat16) for n, c in enumerate(columns)],
            axis=1,
        )
        for copy in first_loads:
            copy.wait()
        part = lax.dot_general(
            normed, first_weights[...], (((1,), (1,)), ((), ())), preferred_element_type=jnp.float32
        ).astype(jnp.bfloat16)
        for o in range(8):
            part_send[o] = part[o * ROWS : (o + 1) * ROWS]

    def send_parts():
        for chip in range(4):
            remote(part_send.at[chip * 2 + 1 - core], part_core.at[chip], (pair_sem.at[0], pair_sem.at[1]), (tp, partner))
        for i, peer in enumerate(dp_peers):
            remote(sq_send.at[peer[1]], sq_recv.at[i], (sq_sem.at[0], sq_sem.at[1]), peer)
        waits.append((part_core, pair_sem.at[0]))
        waits.append((sq_recv, sq_sem.at[0]))

    def send_pair_sums():
        wait_for(part_core, pair_sem.at[1])
        for chip in range(4):
            both = part_send[chip * 2 + core].astype(jnp.float32) + part_core[chip].astype(jnp.float32)
            part_sum[chip] = both.astype(jnp.bfloat16)
        for i, o in enumerate((2, 1, 3)):
            chip = lax.rem(x + o, 4)
            remote(part_sum.at[chip], part_recv.at[i], (part_sem.at[0], part_sem.at[1]), (tp, chip * 2 + core))
        waits.append((part_recv, part_sem.at[0]))

    def first_projected():
        wait_for(sq_recv, sq_sem.at[1])
        square = sq_send[dp]
        for i in range(7):
            square = square + sq_recv[i]
        inv = lax.rsqrt(jnp.sum(square * eye, axis=1, keepdims=True) / D + norm_floor)
        wait_for(part_recv, part_sem.at[1])
        total = part_sum[x].astype(jnp.float32)
        for i in range(3):
            total = total + part_recv[i].astype(jnp.float32)
        return total * inv

    def second_projected():
        squares = jnp.zeros((ROWS, LANES), jnp.float32)
        total = jnp.zeros((6 * HEAD, ROWS), jnp.float32)
        for a in RING8 + (0,):
            d = lax.rem(z + 8 - a, 8)
            wait_for(x_all.at[pl.ds(0, 8 if a else 7)], x_sem.at[a])
            pieces = []
            for c in range(4):
                at = (d * 4 + c) * 2
                piece = jnp.concatenate([x_all[at], x_all[at + 1]], axis=0).astype(jnp.float32)
                squares = squares + piece * piece
                pieces.append((piece * gains[d, 1:2, c * LANES : (c + 1) * LANES]).astype(jnp.bfloat16))
            total = total + lax.dot_general(
                weights[d],
                jnp.concatenate(pieces, axis=1),
                (((1,), (1,)), ((), ())),
                preferred_element_type=jnp.float32,
            )
        inv = lax.rsqrt(jnp.sum(squares, axis=1, keepdims=True) / D + norm_floor)
        return total.T * inv

    def mix(b, projected):
        heads = projected.astype(jnp.bfloat16).astype(jnp.float32)
        both = []
        for n in range(3):
            tile = heads[:, n * LANES : (n + 1) * LANES]
            turned = pltpu.roll(tile, HEAD, 1)
            both.append(jnp.where(low_half, tile, turned))
            both.append(jnp.where(low_half, turned, tile))
        recept, keys, values, decay_part, rate_part, gate_part = both
        base = decay_ref[b : b + 1, :]
        decay = jnp.concatenate([base, base], axis=1) + decay_part
        forget = jnp.exp(-jnp.exp(-jax.nn.softplus(-decay) - 0.5))
        learn = jax.nn.sigmoid(rate_part)
        norm = lax.rsqrt(0.5 * jnp.sum(keys * keys, axis=1, keepdims=True) + 1.0)
        scaled = keys * learn
        with_scaled = 0.5 * jnp.sum(scaled * recept, axis=1, keepdims=True)
        unit = keys * norm
        vec_g[...] = forget * recept - (with_scaled * norm) * unit
        vec_f[...] = forget
        vec_s[...] = scaled
        vec_u[...] = unit * norm
        vec_v[...] = values
        for c in range(4):
            terms = jnp.concatenate([state[b, r] * vec_g[r : r + 1, :] for r in range(c * 8, c * 8 + 8)], axis=0)
            sums = dot(two_terms(terms), by_parity)
            for r in range(8):
                at = c * 8 + r
                chosen = jnp.where(pick, sums[r * ROWS : (r + 1) * ROWS], 0.0)
                read_rows[at : at + 1, :] = jnp.sum(chosen, axis=0, keepdims=True)
        read = read_rows[...] + values * with_scaled
        centre = read - jnp.mean(read, axis=1, keepdims=True)
        normal = centre * lax.rsqrt(jnp.mean(centre * centre, axis=1, keepdims=True) + group_floor)
        gain = group_ref[b : b + 1, :]
        return (normal * jnp.concatenate([gain, gain], axis=1) * jax.nn.sigmoid(gate_part)).astype(jnp.bfloat16)

    own_columns = [lax.rem(x + o, 4) * 2 + core for o in (2, 1, 3, 0)]
    other_columns = [lax.rem(x + o, 4) * 2 + (1 - core) for o in (2, 1, 3, 0)]

    def project_out(b, rows, blocks):
        for d in blocks:
            term = dot(rows, wout[b, d]).astype(jnp.bfloat16)
            for c in range(4):
                for half in range(2):
                    out_send[b, d * 8 + c * 2 + half] = term[
                        half * 16 : (half + 1) * 16, c * LANES : (c + 1) * LANES
                    ]

    def send_out(b):
        for peer in tp_peers:
            remote(out_send.at[b, peer[0]], out_recv.at[b, tp], (out_sem.at[b], out_sem.at[2 + b]), peer)

    def update_state(b):
        for c in range(4):
            terms = jnp.concatenate(
                [
                    jnp.where(pick_own, vec_v[r : r + 1, :], 0.0) - state[b, r] * vec_u[r : r + 1, :]
                    for r in range(c * 8, c * 8 + 8)
                ],
                axis=0,
            )
            sums = dot(two_terms(terms), by_half)
            for r in range(8):
                at = c * 8 + r
                new_state_ref[b, at] = (
                    state[b, at] * vec_f[at : at + 1, :] + sums[r * ROWS : (r + 1) * ROWS] * vec_s[at : at + 1, :]
                )

    def finish_share(b, mine):
        wait_for(out_recv.at[b, pl.ds(0, 63)], out_sem.at[2 + b])
        waits.append((out_recv.at[b, pl.ds(0, 63)], out_sem.at[b]))
        out_recv[b, tp] = out_send[b, tp]
        parts = [out_recv[b, i].astype(jnp.float32) for i in range(4)]
        for i in range(4, 64):
            parts[i % 4] = parts[i % 4] + out_recv[b, i].astype(jnp.float32)
        total = (parts[0] + parts[1]) + (parts[2] + parts[3])
        share[b] = (mine.astype(jnp.float32) + total).astype(jnp.bfloat16)

    def to_partner(b, owner):
        there = wout.at[b, owner]
        remote(there, there, (wout_core_sem.at[b], wout_core_sem.at[2 + b]), (tp, partner))

    def gather_first_wout():
        mine = out_proj_ref.at[0]
        for peer in (far, right, left):
            remote(mine, wout.at[0, dp], (wout_sem.at[0], wout_sem.at[1]), (tp, peer))
        remote(mine, wout.at[0, dp], (wout_core_sem.at[0], wout_core_sem.at[2]), (tp, partner))
        waits.append((wout.at[0, pl.ds(0, 3)], wout_sem.at[0]))

    def pass_first_wout():
        wait_for(wout.at[0, pl.ds(0, 3)], wout_sem.at[1])
        for peer in (far, right, left):
            to_partner(0, peer)
        waits.append((wout.at[0, pl.ds(0, 4)], wout_core_sem.at[0]))

    def gather_second_wout():
        mine = out_proj_ref.at[1]
        remote(mine, wout.at[1, dp], (wout_sem.at[2], wout_sem.at[3]), (tp, left))
        remote(mine, wout.at[1, dp], (wout_sem.at[4], wout_sem.at[5]), (tp, right))
        remote(mine, wout.at[1, dp], (wout_core_sem.at[1], wout_core_sem.at[3]), (tp, partner))
        waits.append((wout.at[1, 0], wout_sem.at[2]))
        waits.append((wout.at[1, 0], wout_sem.at[4]))

    def pass_second_wout():
        from_right = wout.at[1, right]
        wait_for(from_right, wout_sem.at[3])
        remote(from_right, from_right, (wout_sem.at[6], wout_sem.at[7]), (tp, left))
        to_partner(1, right)
        wait_for(wout.at[1, left], wout_sem.at[5])
        to_partner(1, left)
        waits.append((wout.at[1, 0], wout_sem.at[6]))

    def end_second_wout():
        wait_for(wout.at[1, far], wout_sem.at[7])
        to_partner(1, far)
        waits.append((wout.at[1, pl.ds(0, 4)], wout_core_sem.at[1]))

    halves = (pl.ds(0, 3 * HEAD), pl.ds(3 * HEAD, 3 * HEAD))

    def half(owner, n):
        return weights.at[owner, halves[n]]

    def ring_send(owner, n, at, peer):
        there = half(owner, n)
        remote(there, there, (ring_sem.at[at], ring_sem.at[6 + at]), (tp, peer))
        waits.append((half(0, 0), ring_sem.at[at]))

    def core_send(owner):
        there = weights.at[owner]
        remote(there, there, (core_sem.at[0], core_sem.at[1]), (tp, partner))

    def gather_weights():
        for copy in weight_loads:
            copy.wait()
        ring_send(dp, 0, 0, right)
        ring_send(dp, 1, 2, left)
        ring_send(dp, 1, 1, right)
        ring_send(dp, 0, 3, left)
        core_send(dp)

    def pass_weights():
        wait_for(half(right, 1), ring_sem.at[8])
        ring_send(right, 1, 5, left)
        wait_for(half(left, 0), ring_sem.at[6])
        ring_send(left, 0, 4, right)

    def pass_to_partner():
        wait_for(half(right, 0), ring_sem.at[9])
        core_send(right)
        wait_for(half(left, 1), ring_sem.at[7])
        core_send(left)

    def end_weights():
        wait_for(half(far, 0), ring_sem.at[10])
        wait_for(half(far, 1), ring_sem.at[11])
        core_send(far)
        waits.append((weights.at[pl.ds(0, 4)], core_sem.at[0]))

    pl.semaphore_wait(barrier, 11)
    gather_first_wout()
    tell(near_sem, beside(1))
    tokens_load.wait()
    first_parts()
    send_parts()
    pl.semaphore_wait(near_sem, 4)
    tell(line_sem, beside(2))
    send_pair_sums()
    pl.semaphore_wait(line_sem, 4)
    tell(row_sem, z_peers)
    for peer in dp_peers:
        remote(gains.at[dp], gains.at[dp], (gain_sem.at[0], gain_sem.at[1]), peer)
    waits.append((gains.at[pl.ds(0, 7)], gain_sem.at[0]))
    at_column = pl.ds(pl.multiple_of(column * LANES, LANES), LANES)

    def at_rows(owner):
        return pl.ds(pl.multiple_of(owner * ROWS + half_row * 16, 16), 16)

    @pl.when(owns_columns)
    def _():
        for peer in dp_peers:
            remote(tokens.at[at_rows(peer[1]), at_column], residue, (residue_sem.at[0], residue_sem.at[1]), peer)
        residue[...] = tokens[at_rows(dp), at_column]

    gather_weights()
    gather_second_wout()
    pass_first_wout()
    projected = first_projected()
    for copy in small_loads + [state_load]:
        copy.wait()
    mixed = mix(0, projected)[:, :HEAD]
    pl.semaphore_wait(row_sem, 7)
    tell(plane_sem, dp_peers)
    for copy in wout_loads:
        copy.wait()
    project_out(0, mixed, own_columns)
    wait_for(wout.at[0, pl.ds(0, 4)], wout_core_sem.at[2])
    project_out(0, mixed, other_columns)
    send_out(0)
    update_state(0)
    pass_weights()
    pass_to_partner()

    @pl.when(jnp.logical_not(owns_columns))
    def _():
        wait_for(residue, residue_sem.at[1])

    finish_share(0, residue[...])
    x_all[tp] = share[0]
    for peer, (a, _) in zip(tp_peers, TP_OFFSETS):
        remote(share.at[0], x_all.at[tp], (x_sem.at[8], x_sem.at[a]), peer)
    waits.append((x_all.at[pl.ds(0, 63)], x_sem.at[8]))
    pass_second_wout()
    end_weights()
    end_second_wout()
    wait_for(gains.at[pl.ds(0, 7)], gain_sem.at[1])
    pl.semaphore_wait(plane_sem, 7)
    wait_for(weights.at[pl.ds(0, 4)], core_sem.at[1])

    mixed = mix(1, second_projected())[:, :HEAD]
    wait_for(wout.at[1, pl.ds(0, 4)], wout_core_sem.at[3])
    project_out(1, mixed, range(8))
    send_out(1)
    update_state(1)
    finish_share(1, share[0])
    slot = (dp * 2 + half_row) * 4 + column

    @pl.when(jnp.logical_not(owns_columns))
    def _():
        remote(share.at[1], x_last.at[slot], (last_sem.at[2], last_sem.at[1]), (tp, z))

    @pl.when(owns_columns)
    def _():
        load(share.at[1], x_last.at[slot], last_sem.at[1])

    for peer in tp_peers:
        remote(share.at[1], x_last.at[slot], (last_sem.at[0], last_sem.at[1]), (peer[0], z))
    waits.append((x_last.at[pl.ds(0, 63)], last_sem.at[0]))
    wait_for(x_last, last_sem.at[1])
    for g in range(16):
        for c in range(4):
            next_ref[g * 16 : (g + 1) * 16, c * LANES : (c + 1) * LANES] = x_last[g * 4 + c]

    @pl.when(jnp.logical_not(owns_columns))
    def _():
        wait_for(share.at[1], last_sem.at[2])

    @pl.when(owns_columns)
    def _():
        wait_for(x_last.at[pl.ds(0, 7)], residue_sem.at[0])

    for ref, sem in waits:
        wait_for(ref, sem)


def write_out(next_ref, state_ref, next_out, state_out, sems):
    copies = [
        pltpu.make_async_copy(src, dst, sems.at[n])
        for n, (src, dst) in enumerate(((state_ref, state_out), (next_ref, next_out)))
    ]
    for copy in copies:
        copy.start()
    for copy in copies:
        copy.wait()


def shards(
    tokens,
    norm_gain,
    receptance,
    key_proj,
    value_proj,
    decay_proj,
    rate_proj,
    gate_proj,
    decay_base,
    group_gain,
    output_proj,
    state,
):
    flat = [jnp.swapaxes(w, 1, 2) for w in (receptance, key_proj, value_proj, decay_proj, rate_proj, gate_proj)]
    remote = pl.BlockSpec(memory_space=pltpu.HBM)
    local = pl.BlockSpec(memory_space=pltpu.VMEM)
    f32, bf16 = jnp.float32, jnp.bfloat16
    dma = pltpu.SemaphoreType.DMA

    current, updated = pl.pallas_call(
        body,
        out_shape=(
            pltpu.VMEM((256, WIDE), bf16),
            pltpu.VMEM((LAYERS, ROWS, 32, LANES), f32),
        ),
        in_specs=[remote] * 12,
        out_specs=(local, local),
        scratch_shapes=[
            pltpu.VMEM((256, WIDE), bf16),
            pltpu.VMEM((6 * HEAD, WIDE), bf16),
            pltpu.VMEM((8, 6 * HEAD, WIDE), bf16),
            pltpu.VMEM((LAYERS, 8, HEAD, WIDE), bf16),
            pltpu.VMEM((8, LAYERS, WIDE), f32),
            pltpu.VMEM((LAYERS, HEAD), f32),
            pltpu.VMEM((LAYERS, HEAD), f32),
            pltpu.VMEM((16, LANES), bf16),
            pltpu.VMEM((LAYERS, ROWS, 32, LANES), f32),
            pltpu.VMEM((8, ROWS, 6 * HEAD), bf16),
            pltpu.VMEM((4, ROWS, 6 * HEAD), bf16),
            pltpu.VMEM((4, ROWS, 6 * HEAD), bf16),
            pltpu.VMEM((3, ROWS, 6 * HEAD), bf16),
            pltpu.VMEM((8, 1, LANES), f32),
            pltpu.VMEM((7, 1, LANES), f32),
            pltpu.VMEM((LAYERS, 64, 16, LANES), bf16),
            pltpu.VMEM((LAYERS, 64, 16, LANES), bf16),
            pltpu.VMEM((LAYERS, 16, LANES), bf16),
            pltpu.VMEM((64, 16, LANES), bf16),
            pltpu.VMEM((64, 16, LANES), bf16),
        ]
        + [pltpu.VMEM((ROWS, LANES), f32)] * 6
        + [dma((10,)), dma((9,)), dma((2,)), dma((2,)), dma((2,)), dma((4,)), dma((9,)), dma((2,)), dma((2,))]
        + [dma((8,)), dma((4,)), dma((12,)), dma((2,)), dma((3,))]
        + [pltpu.SemaphoreType.REGULAR] * 4,
        compiler_params=pltpu.CompilerParams(
            collective_id=0, has_side_effects=True, vmem_limit_bytes=32 * 1024 * 1024
        ),
        name="blocks",
    )(
        *[
            pltpu.with_memory_space_constraint(a, pltpu.HBM)
            for a in (
                tokens,
                norm_gain,
                *flat,
                decay_base,
                group_gain,
                output_proj,
                state.reshape(LAYERS, ROWS, 32, LANES),
            )
        ]
    )
    current, updated = pl.pallas_call(
        write_out,
        out_shape=(
            jax.ShapeDtypeStruct((256, WIDE), bf16),
            jax.ShapeDtypeStruct((LAYERS, ROWS, 32, LANES), f32),
        ),
        in_specs=[local, local],
        out_specs=(remote, remote),
        scratch_shapes=[dma((2,))],
        name="write_out",
    )(*[pltpu.with_memory_space_constraint(a, pltpu.VMEM) for a in (current, updated)])
    return (current, updated.reshape(LAYERS, ROWS, 1, HEAD * HEAD))


def solution(mesh):
    return jax.shard_map(
        shards,
        mesh=mesh,
        in_specs=(
            P(None, "dp"),
            P(None, "dp"),
            P(None, "dp", "tp"),
            P(None, "dp", "tp"),
            P(None, "dp", "tp"),
            P(None, "dp", "tp"),
            P(None, "dp", "tp"),
            P(None, "dp", "tp"),
            P(None, "tp"),
            P(None, "tp"),
            P(None, "tp", "dp"),
            P(None, "dp", "tp", None),
        ),
        out_specs=(P(None, "dp"), P(None, "dp", "tp", None)),
        check_vma=False,
    )
```

```python
import jax
import jax.numpy as jnp
from jax import lax
from jax.experimental import pallas as pl
from jax.experimental.pallas import tpu as pltpu
from jax.sharding import PartitionSpec as P

D = 4096
HEAD = 64
LAYERS = 2
ROWS = 32
WIDE = 512
LANES = 128

norm_floor = 0.1
group_floor = 0.5

MESH = pl.DeviceIdType.MESH
RING8 = (4, 3, 5, 2, 6, 1, 7)
TP_OFFSETS = sorted(
    ((a, b) for a in range(8) for b in range(8) if (a, b) != (0, 0)),
    key=lambda ab: -(min(ab[0], 8 - ab[0]) + min(ab[1], 8 - ab[1])),
)


def iota(shape, dim):
    return lax.broadcasted_iota(jnp.int32, shape, dim)


def two_terms(x):
    high = x.astype(jnp.bfloat16)
    low = (x - high.astype(jnp.float32)).astype(jnp.bfloat16)
    return jnp.concatenate([high, low], axis=1)


def dot(a, b):
    return jnp.dot(a, b, preferred_element_type=jnp.float32)


def contract(a, b):
    return lax.dot_general(a, b, (((1,), (1,)), ((), ())), preferred_element_type=jnp.float32)


def wait_for(ref, sem):
    pltpu.make_async_copy(ref, ref, sem).wait()


def body(
    tokens_ref,
    gain_in,
    w0,
    w1,
    w2,
    w3,
    w4,
    w5,
    decay_in,
    group_in,
    out_proj_ref,
    state_ref,
    next_ref,
    new_state_ref,
    tokens,
    first_weights,
    weights,
    wout,
    gains,
    decay_ref,
    group_ref,
    residue,
    state,
    part_send,
    part_core,
    part_sum,
    part_recv,
    sq_send,
    sq_recv,
    out_send,
    out_recv,
    share,
    x_all,
    x_last,
    vec_g,
    vec_f,
    vec_s,
    vec_u,
    vec_v,
    read_rows,
    load_sem,
    late_sem,
    pair_sem,
    part_sem,
    sq_sem,
    out_sem,
    x_sem,
    gain_sem,
    residue_sem,
    wout_sem,
    wout_core_sem,
    ring_sem,
    core_sem,
    last_sem,
    near_sem,
    line_sem,
    row_sem,
    plane_sem,
):
    tp = lax.axis_index("tp")
    dp = lax.axis_index("dp")
    z = tp // 8
    y = lax.rem(tp, 8)
    x = dp // 2
    core = lax.rem(dp, 2)
    dp_peers = [(tp, lax.rem(dp + o, 8)) for o in RING8]
    z_peers = [(lax.rem(z + o, 8) * 8 + y, dp) for o in RING8]
    tp_peers = [(lax.rem(z + a, 8) * 8 + lax.rem(y + b, 8), dp) for a, b in TP_OFFSETS]
    right, far, left = (lax.rem(x + o, 4) * 2 + core for o in (1, 2, 3))
    partner = x * 2 + (1 - core)
    owns_columns = dp == z
    half_row = lax.rem(y, 2)
    column = y // 2

    def remote(src, dst, sems, peer):
        copy = pltpu.make_async_remote_copy(
            src_ref=src, dst_ref=dst, send_sem=sems[0], recv_sem=sems[1], device_id=peer, device_id_type=MESH
        )
        copy.start()
        return copy

    def beside(o):
        return [(z * 8 + lax.rem(y + k, 8), dp) for k in (o, 8 - o)] + [
            (lax.rem(z + k, 8) * 8 + y, dp) for k in (o, 8 - o)
        ]

    def tell(sem, peers):
        for peer in peers:
            pl.semaphore_signal(sem, inc=1, device_id=peer, device_id_type=MESH)

    barrier = pltpu.get_barrier_semaphore()
    tell(barrier, dp_peers + beside(1))

    def load(src, dst, sem):
        copy = pltpu.make_async_copy(src, dst, sem)
        copy.start()
        return copy

    tokens_load = load(tokens_ref, tokens, load_sem.at[0])
    gain_load = load(gain_in, gains.at[dp], load_sem.at[7])
    small_loads = [load(decay_in, decay_ref, load_sem.at[8]), load(group_in, group_ref, load_sem.at[9])]
    projections = (w0, w1, w2, w3, w4, w5)
    first_loads = [
        load(w.at[0], first_weights.at[pl.ds(n * HEAD, HEAD)], load_sem.at[n + 1]) for n, w in enumerate(projections)
    ]
    wout_loads = [load(out_proj_ref.at[b], wout.at[b, dp], late_sem.at[7 + b]) for b in range(LAYERS)]
    state_load = load(state_ref, state, late_sem.at[0])
    weight_loads = [
        load(w.at[1], weights.at[dp, pl.ds(n * HEAD, HEAD)], late_sem.at[n + 1]) for n, w in enumerate(projections)
    ]

    lane = iota((ROWS, LANES), 1)
    row = iota((ROWS, LANES), 0)
    low_half = lane < HEAD
    eye = (lane == row).astype(jnp.float32)
    pick = (lane % HEAD) // 2 == row
    pick_own = lane % HEAD == 2 * row + lane // HEAD
    ones = jnp.full((2 * LANES, LANES), 1.0, jnp.bfloat16)
    k_of = iota((2 * LANES, LANES), 0)
    l_of = iota((2 * LANES, LANES), 1)
    by_parity = ((k_of // HEAD) % 2 == l_of % 2).astype(jnp.float32).astype(jnp.bfloat16)
    by_half = ((k_of // HEAD) % 2 == l_of // HEAD).astype(jnp.float32).astype(jnp.bfloat16)

    waits = []

    def first_parts():
        columns = [tokens[:, c * LANES : (c + 1) * LANES].astype(jnp.float32) for c in range(4)]
        squares = columns[0] * columns[0]
        for c in columns[1:]:
            squares = squares + c * c
        totals = dot(two_terms(squares), ones)
        for o in range(8):
            sq_send[o] = jnp.sum(totals[o * ROWS : (o + 1) * ROWS] * eye, axis=0, keepdims=True)
        gain_load.wait()
        normed = jnp.concatenate(
            [(c * gains[dp, 0:1, n * LANES : (n + 1) * LANES]).astype(jnp.bfloat16) for n, c in enumerate(columns)],
            axis=1,
        )
        for copy in first_loads:
            copy.wait()
        part = contract(normed, first_weights[...]).astype(jnp.bfloat16)
        for o in range(8):
            part_send[o] = part[o * ROWS : (o + 1) * ROWS]

    def send_parts():
        for chip in range(4):
            remote(part_send.at[chip * 2 + 1 - core], part_core.at[chip], (pair_sem.at[0], pair_sem.at[1]), (tp, partner))
        for i, peer in enumerate(dp_peers):
            remote(sq_send.at[peer[1]], sq_recv.at[i], (sq_sem.at[0], sq_sem.at[1]), peer)
        waits.append((part_core, pair_sem.at[0]))
        waits.append((sq_recv, sq_sem.at[0]))

    def send_pair_sums():
        wait_for(part_core, pair_sem.at[1])
        for chip in range(4):
            both = part_send[chip * 2 + core].astype(jnp.float32) + part_core[chip].astype(jnp.float32)
            part_sum[chip] = both.astype(jnp.bfloat16)
        for i, o in enumerate((2, 1, 3)):
            chip = lax.rem(x + o, 4)
            remote(part_sum.at[chip], part_recv.at[i], (part_sem.at[0], part_sem.at[1]), (tp, chip * 2 + core))
        waits.append((part_recv, part_sem.at[0]))

    def first_projected():
        wait_for(sq_recv, sq_sem.at[1])
        square = sq_send[dp]
        for i in range(7):
            square = square + sq_recv[i]
        inv = lax.rsqrt(jnp.sum(square * eye, axis=1, keepdims=True) / D + norm_floor)
        wait_for(part_recv, part_sem.at[1])
        total = part_sum[x].astype(jnp.float32)
        for i in range(3):
            total = total + part_recv[i].astype(jnp.float32)
        return total * inv

    def second_projected():
        squares = jnp.zeros((ROWS, LANES), jnp.float32)
        total = jnp.zeros((6 * HEAD, ROWS), jnp.float32)
        held = jnp.zeros((ROWS, 6 * HEAD), jnp.float32)
        arrivals = ((4, 3, 5, 2), (6, 1, 7, 0))
        for a in arrivals[0] + arrivals[1]:
            d = lax.rem(z + 8 - a, 8)
            for group in arrivals:
                if a == group[0]:
                    for other in group:
                        wait_for(x_all.at[pl.ds(0, 8 if other else 7)], x_sem.at[other])
            pieces = []
            for c in range(4):
                at = (d * 4 + c) * 2
                piece = jnp.concatenate([x_all[at], x_all[at + 1]], axis=0).astype(jnp.float32)
                squares = squares + piece * piece
                pieces.append((piece * gains[d, 1:2, c * LANES : (c + 1) * LANES]).astype(jnp.bfloat16))
            total = total + contract(weights[d, :, 0 : 2 * LANES], jnp.concatenate(pieces[:2], axis=1))
            held = held + contract(jnp.concatenate(pieces[2:], axis=1), weights[d, :, 2 * LANES :])
        inv = lax.rsqrt(jnp.sum(squares, axis=1, keepdims=True) / D + norm_floor)
        return (total.T + held) * inv

    def mix(b, projected):
        heads = projected.astype(jnp.bfloat16).astype(jnp.float32)
        both = []
        for n in range(3):
            tile = heads[:, n * LANES : (n + 1) * LANES]
            turned = pltpu.roll(tile, HEAD, 1)
            both.append(jnp.where(low_half, tile, turned))
            both.append(jnp.where(low_half, turned, tile))
        recept, keys, values, decay_part, rate_part, gate_part = both
        base = decay_ref[b : b + 1, :]
        decay = jnp.concatenate([base, base], axis=1) + decay_part
        forget = jnp.exp(-jnp.exp(-jax.nn.softplus(-decay) - 0.5))
        learn = jax.nn.sigmoid(rate_part)
        norm = lax.rsqrt(0.5 * jnp.sum(keys * keys, axis=1, keepdims=True) + 1.0)
        scaled = keys * learn
        with_scaled = 0.5 * jnp.sum(scaled * recept, axis=1, keepdims=True)
        unit = keys * norm
        vec_g[...] = forget * recept - (with_scaled * norm) * unit
        vec_f[...] = forget
        vec_s[...] = scaled
        vec_u[...] = unit * norm
        vec_v[...] = values
        for c in range(4):
            terms = jnp.concatenate([state[b, r] * vec_g[r : r + 1, :] for r in range(c * 8, c * 8 + 8)], axis=0)
            sums = dot(two_terms(terms), by_parity)
            for r in range(8):
                at = c * 8 + r
                chosen = jnp.where(pick, sums[r * ROWS : (r + 1) * ROWS], 0.0)
                read_rows[at : at + 1, :] = jnp.sum(chosen, axis=0, keepdims=True)
        read = read_rows[...] + values * with_scaled
        centre = read - jnp.mean(read, axis=1, keepdims=True)
        normal = centre * lax.rsqrt(jnp.mean(centre * centre, axis=1, keepdims=True) + group_floor)
        gain = group_ref[b : b + 1, :]
        return (normal * jnp.concatenate([gain, gain], axis=1) * jax.nn.sigmoid(gate_part)).astype(jnp.bfloat16)

    own_columns = [lax.rem(x + o, 4) * 2 + core for o in (2, 1, 3, 0)]
    other_columns = [lax.rem(x + o, 4) * 2 + (1 - core) for o in (2, 1, 3, 0)]

    def project_out(b, rows, blocks):
        for d in blocks:
            term = dot(rows, wout[b, d]).astype(jnp.bfloat16)
            for c in range(4):
                for half in range(2):
                    out_send[b, d * 8 + c * 2 + half] = term[
                        half * 16 : (half + 1) * 16, c * LANES : (c + 1) * LANES
                    ]

    def send_out(b):
        for peer in tp_peers:
            remote(out_send.at[b, peer[0]], out_recv.at[b, tp], (out_sem.at[b], out_sem.at[2 + b]), peer)

    def update_state(b):
        for c in range(4):
            terms = jnp.concatenate(
                [
                    jnp.where(pick_own, vec_v[r : r + 1, :], 0.0) - state[b, r] * vec_u[r : r + 1, :]
                    for r in range(c * 8, c * 8 + 8)
                ],
                axis=0,
            )
            sums = dot(two_terms(terms), by_half)
            for r in range(8):
                at = c * 8 + r
                new_state_ref[b, at] = (
                    state[b, at] * vec_f[at : at + 1, :] + sums[r * ROWS : (r + 1) * ROWS] * vec_s[at : at + 1, :]
                )

    def finish_share(b, mine):
        wait_for(out_recv.at[b, pl.ds(0, 63)], out_sem.at[2 + b])
        waits.append((out_recv.at[b, pl.ds(0, 63)], out_sem.at[b]))
        out_recv[b, tp] = out_send[b, tp]
        parts = [out_recv[b, i].astype(jnp.float32) for i in range(4)]
        for i in range(4, 64):
            parts[i % 4] = parts[i % 4] + out_recv[b, i].astype(jnp.float32)
        total = (parts[0] + parts[1]) + (parts[2] + parts[3])
        share[b] = (mine.astype(jnp.float32) + total).astype(jnp.bfloat16)

    def to_partner(b, owner):
        there = wout.at[b, owner]
        remote(there, there, (wout_core_sem.at[b], wout_core_sem.at[2 + b]), (tp, partner))

    def gather_first_wout():
        mine = out_proj_ref.at[0]
        for peer in (far, right, left):
            remote(mine, wout.at[0, dp], (wout_sem.at[0], wout_sem.at[1]), (tp, peer))
        remote(mine, wout.at[0, dp], (wout_core_sem.at[0], wout_core_sem.at[2]), (tp, partner))
        waits.append((wout.at[0, pl.ds(0, 3)], wout_sem.at[0]))

    def pass_first_wout():
        wait_for(wout.at[0, pl.ds(0, 3)], wout_sem.at[1])
        for peer in (far, right, left):
            to_partner(0, peer)
        waits.append((wout.at[0, pl.ds(0, 4)], wout_core_sem.at[0]))

    def gather_second_wout():
        mine = out_proj_ref.at[1]
        remote(mine, wout.at[1, dp], (wout_sem.at[2], wout_sem.at[3]), (tp, left))
        remote(mine, wout.at[1, dp], (wout_sem.at[4], wout_sem.at[5]), (tp, right))
        remote(mine, wout.at[1, dp], (wout_core_sem.at[1], wout_core_sem.at[3]), (tp, partner))
        waits.append((wout.at[1, 0], wout_sem.at[2]))
        waits.append((wout.at[1, 0], wout_sem.at[4]))

    def pass_second_wout():
        from_right = wout.at[1, right]
        wait_for(from_right, wout_sem.at[3])
        remote(from_right, from_right, (wout_sem.at[6], wout_sem.at[7]), (tp, left))
        to_partner(1, right)
        wait_for(wout.at[1, left], wout_sem.at[5])
        to_partner(1, left)
        waits.append((wout.at[1, 0], wout_sem.at[6]))

    def end_second_wout():
        wait_for(wout.at[1, far], wout_sem.at[7])
        to_partner(1, far)
        waits.append((wout.at[1, pl.ds(0, 4)], wout_core_sem.at[1]))

    halves = (pl.ds(0, 192), pl.ds(192, 192))

    def half(owner, n):
        return weights.at[owner, halves[n]]

    def ring_send(owner, n, at, peer):
        there = half(owner, n)
        remote(there, there, (ring_sem.at[at], ring_sem.at[6 + at]), (tp, peer))
        waits.append((half(0, n), ring_sem.at[at]))

    def core_send(owner):
        there = weights.at[owner]
        remote(there, there, (core_sem.at[0], core_sem.at[1]), (tp, partner))

    def gather_weights():
        for copy in weight_loads:
            copy.wait()
        ring_send(dp, 0, 0, right)
        ring_send(dp, 1, 2, left)
        ring_send(dp, 1, 1, right)
        ring_send(dp, 0, 3, left)
        core_send(dp)

    def pass_weights():
        wait_for(half(right, 1), ring_sem.at[8])
        ring_send(right, 1, 5, left)
        wait_for(half(left, 0), ring_sem.at[6])
        ring_send(left, 0, 4, right)

    def pass_to_partner():
        wait_for(half(right, 0), ring_sem.at[9])
        core_send(right)
        wait_for(half(left, 1), ring_sem.at[7])
        core_send(left)

    def end_weights():
        wait_for(half(far, 0), ring_sem.at[10])
        wait_for(half(far, 1), ring_sem.at[11])
        core_send(far)
        waits.append((weights.at[pl.ds(0, 4)], core_sem.at[0]))

    pl.semaphore_wait(barrier, 11)
    gather_first_wout()
    tell(near_sem, beside(1))
    tokens_load.wait()
    first_parts()
    send_parts()
    send_pair_sums()
    for peer in dp_peers:
        remote(gains.at[dp], gains.at[dp], (gain_sem.at[0], gain_sem.at[1]), peer)
    waits.append((gains.at[pl.ds(0, 7)], gain_sem.at[0]))
    at_column = pl.ds(pl.multiple_of(column * LANES, LANES), LANES)

    def at_rows(owner):
        return pl.ds(pl.multiple_of(owner * ROWS + half_row * 16, 16), 16)

    @pl.when(owns_columns)
    def _():
        for peer in dp_peers:
            remote(tokens.at[at_rows(peer[1]), at_column], residue, (residue_sem.at[0], residue_sem.at[1]), peer)
        residue[...] = tokens[at_rows(dp), at_column]

    pl.semaphore_wait(near_sem, 4)
    tell(line_sem, beside(2))
    pl.semaphore_wait(line_sem, 4)
    tell(row_sem, z_peers)
    gather_weights()
    gather_second_wout()
    pass_first_wout()
    projected = first_projected()
    for copy in small_loads + [state_load]:
        copy.wait()
    mixed = mix(0, projected)[:, :HEAD]
    pl.semaphore_wait(row_sem, 7)
    tell(plane_sem, dp_peers)
    for copy in wout_loads:
        copy.wait()
    project_out(0, mixed, own_columns)
    wait_for(wout.at[0, pl.ds(0, 4)], wout_core_sem.at[2])
    project_out(0, mixed, other_columns)
    send_out(0)
    update_state(0)
    pass_weights()
    pass_to_partner()

    @pl.when(jnp.logical_not(owns_columns))
    def _():
        wait_for(residue, residue_sem.at[1])

    finish_share(0, residue[...])
    x_all[tp] = share[0]
    for peer, (a, _) in zip(tp_peers, TP_OFFSETS):
        remote(share.at[0], x_all.at[tp], (x_sem.at[8], x_sem.at[a]), peer)
    waits.append((x_all.at[pl.ds(0, 63)], x_sem.at[8]))
    pass_second_wout()
    end_weights()
    end_second_wout()
    wait_for(gains.at[pl.ds(0, 7)], gain_sem.at[1])
    pl.semaphore_wait(plane_sem, 7)
    wait_for(weights.at[pl.ds(0, 4)], core_sem.at[1])

    mixed = mix(1, second_projected())[:, :HEAD]
    wait_for(wout.at[1, pl.ds(0, 4)], wout_core_sem.at[3])
    project_out(1, mixed, range(8))
    send_out(1)
    update_state(1)
    finish_share(1, share[0])
    slot = (dp * 2 + half_row) * 4 + column

    @pl.when(jnp.logical_not(owns_columns))
    def _():
        remote(share.at[1], x_last.at[slot], (last_sem.at[2], last_sem.at[1]), (tp, z))

    @pl.when(owns_columns)
    def _():
        load(share.at[1], x_last.at[slot], last_sem.at[1])

    for peer in tp_peers:
        remote(share.at[1], x_last.at[slot], (last_sem.at[0], last_sem.at[1]), (peer[0], z))
    waits.append((x_last.at[pl.ds(0, 63)], last_sem.at[0]))
    wait_for(x_last, last_sem.at[1])
    for g in range(16):
        for c in range(4):
            next_ref[g * 16 : (g + 1) * 16, c * LANES : (c + 1) * LANES] = x_last[g * 4 + c]

    @pl.when(jnp.logical_not(owns_columns))
    def _():
        wait_for(share.at[1], last_sem.at[2])

    @pl.when(owns_columns)
    def _():
        wait_for(x_last.at[pl.ds(0, 7)], residue_sem.at[0])

    for ref, sem in waits:
        wait_for(ref, sem)


def write_out(next_ref, state_ref, next_out, state_out, sems):
    copies = [
        pltpu.make_async_copy(src, dst, sems.at[n])
        for n, (src, dst) in enumerate(((state_ref, state_out), (next_ref, next_out)))
    ]
    for copy in copies:
        copy.start()
    for copy in copies:
        copy.wait()


def shards(
    tokens,
    norm_gain,
    receptance,
    key_proj,
    value_proj,
    decay_proj,
    rate_proj,
    gate_proj,
    decay_base,
    group_gain,
    output_proj,
    state,
):
    flat = [jnp.swapaxes(w, 1, 2) for w in (receptance, key_proj, value_proj, decay_proj, rate_proj, gate_proj)]
    remote = pl.BlockSpec(memory_space=pltpu.HBM)
    local = pl.BlockSpec(memory_space=pltpu.VMEM)
    f32, bf16 = jnp.float32, jnp.bfloat16
    dma = pltpu.SemaphoreType.DMA

    current, updated = pl.pallas_call(
        body,
        out_shape=(
            pltpu.VMEM((256, WIDE), bf16),
            pltpu.VMEM((LAYERS, ROWS, 32, LANES), f32),
        ),
        in_specs=[remote] * 12,
        out_specs=(local, local),
        scratch_shapes=[
            pltpu.VMEM((256, WIDE), bf16),
            pltpu.VMEM((6 * HEAD, WIDE), bf16),
            pltpu.VMEM((8, 6 * HEAD, WIDE), bf16),
            pltpu.VMEM((LAYERS, 8, HEAD, WIDE), bf16),
            pltpu.VMEM((8, LAYERS, WIDE), f32),
            pltpu.VMEM((LAYERS, HEAD), f32),
            pltpu.VMEM((LAYERS, HEAD), f32),
            pltpu.VMEM((16, LANES), bf16),
            pltpu.VMEM((LAYERS, ROWS, 32, LANES), f32),
            pltpu.VMEM((8, ROWS, 6 * HEAD), bf16),
            pltpu.VMEM((4, ROWS, 6 * HEAD), bf16),
            pltpu.VMEM((4, ROWS, 6 * HEAD), bf16),
            pltpu.VMEM((3, ROWS, 6 * HEAD), bf16),
            pltpu.VMEM((8, 1, LANES), f32),
            pltpu.VMEM((7, 1, LANES), f32),
            pltpu.VMEM((LAYERS, 64, 16, LANES), bf16),
            pltpu.VMEM((LAYERS, 64, 16, LANES), bf16),
            pltpu.VMEM((LAYERS, 16, LANES), bf16),
            pltpu.VMEM((64, 16, LANES), bf16),
            pltpu.VMEM((64, 16, LANES), bf16),
        ]
        + [pltpu.VMEM((ROWS, LANES), f32)] * 6
        + [dma((10,)), dma((9,)), dma((2,)), dma((2,)), dma((2,)), dma((4,)), dma((9,)), dma((2,)), dma((2,))]
        + [dma((8,)), dma((4,)), dma((12,)), dma((2,)), dma((3,))]
        + [pltpu.SemaphoreType.REGULAR] * 4,
        compiler_params=pltpu.CompilerParams(
            collective_id=0, has_side_effects=True, vmem_limit_bytes=32 * 1024 * 1024
        ),
        name="blocks",
    )(
        *[
            pltpu.with_memory_space_constraint(a, pltpu.HBM)
            for a in (
                tokens,
                norm_gain,
                *flat,
                decay_base,
                group_gain,
                output_proj,
                state.reshape(LAYERS, ROWS, 32, LANES),
            )
        ]
    )
    current, updated = pl.pallas_call(
        write_out,
        out_shape=(
            jax.ShapeDtypeStruct((256, WIDE), bf16),
            jax.ShapeDtypeStruct((LAYERS, ROWS, 32, LANES), f32),
        ),
        in_specs=[local, local],
        out_specs=(remote, remote),
        scratch_shapes=[dma((2,))],
        name="write_out",
    )(*[pltpu.with_memory_space_constraint(a, pltpu.VMEM) for a in (current, updated)])
    return (current, updated.reshape(LAYERS, ROWS, 1, HEAD * HEAD))


def solution(mesh):
    return jax.shard_map(
        shards,
        mesh=mesh,
        in_specs=(
            P(None, "dp"),
            P(None, "dp"),
            P(None, "dp", "tp"),
            P(None, "dp", "tp"),
            P(None, "dp", "tp"),
            P(None, "dp", "tp"),
            P(None, "dp", "tp"),
            P(None, "dp", "tp"),
            P(None, "tp"),
            P(None, "tp"),
            P(None, "tp", "dp"),
            P(None, "dp", "tp", None),
        ),
        out_specs=(P(None, "dp"), P(None, "dp", "tp", None)),
        check_vma=False,
    )
```

```python
import jax
import jax.numpy as jnp
from jax import lax
from jax.experimental import pallas as pl
from jax.experimental.pallas import tpu as pltpu
from jax.sharding import PartitionSpec as P

D = 4096
HEAD = 64
LAYERS = 2
ROWS = 32
WIDE = 512
LANES = 128

norm_floor = 0.1
group_floor = 0.5

MESH = pl.DeviceIdType.MESH
RING8 = (4, 3, 5, 2, 6, 1, 7)
TP_OFFSETS = sorted(
    ((a, b) for a in range(8) for b in range(8) if (a, b) != (0, 0)),
    key=lambda ab: -(min(ab[0], 8 - ab[0]) + min(ab[1], 8 - ab[1])),
)


def iota(shape, dim):
    return lax.broadcasted_iota(jnp.int32, shape, dim)


def two_terms(x):
    high = x.astype(jnp.bfloat16)
    low = (x - high.astype(jnp.float32)).astype(jnp.bfloat16)
    return jnp.concatenate([high, low], axis=1)


def dot(a, b):
    return jnp.dot(a, b, preferred_element_type=jnp.float32)


def contract(a, b):
    return lax.dot_general(a, b, (((1,), (1,)), ((), ())), preferred_element_type=jnp.float32)


def wait_for(ref, sem):
    pltpu.make_async_copy(ref, ref, sem).wait()


def body(
    tokens_ref,
    gain_in,
    w0,
    w1,
    w2,
    w3,
    w4,
    w5,
    decay_in,
    group_in,
    out_proj_ref,
    state_ref,
    next_ref,
    new_state_ref,
    tokens,
    first_weights,
    weights,
    wout,
    gains,
    decay_ref,
    group_ref,
    residue,
    state,
    part_send,
    part_core,
    part_sum,
    part_recv,
    sq_send,
    sq_recv,
    out_send,
    out_recv,
    share,
    x_all,
    x_last,
    vec_g,
    vec_f,
    vec_s,
    vec_u,
    vec_v,
    read_rows,
    load_sem,
    late_sem,
    pair_sem,
    part_sem,
    sq_sem,
    out_sem,
    x_sem,
    gain_sem,
    residue_sem,
    wout_sem,
    wout_core_sem,
    ring_sem,
    core_sem,
    last_sem,
    near_sem,
    line_sem,
    row_sem,
    plane_sem,
):
    tp = lax.axis_index("tp")
    dp = lax.axis_index("dp")
    z = tp // 8
    y = lax.rem(tp, 8)
    x = dp // 2
    core = lax.rem(dp, 2)
    dp_peers = [(tp, lax.rem(dp + o, 8)) for o in RING8]
    z_peers = [(lax.rem(z + o, 8) * 8 + y, dp) for o in RING8]
    tp_peers = [(lax.rem(z + a, 8) * 8 + lax.rem(y + b, 8), dp) for a, b in TP_OFFSETS]
    right, far, left = (lax.rem(x + o, 4) * 2 + core for o in (1, 2, 3))
    partner = x * 2 + (1 - core)
    owns_columns = dp == z
    half_row = lax.rem(y, 2)
    column = y // 2

    def remote(src, dst, sems, peer):
        copy = pltpu.make_async_remote_copy(
            src_ref=src, dst_ref=dst, send_sem=sems[0], recv_sem=sems[1], device_id=peer, device_id_type=MESH
        )
        copy.start()
        return copy

    def beside(o):
        return [(z * 8 + lax.rem(y + k, 8), dp) for k in (o, 8 - o)] + [
            (lax.rem(z + k, 8) * 8 + y, dp) for k in (o, 8 - o)
        ]

    def tell(sem, peers):
        for peer in peers:
            pl.semaphore_signal(sem, inc=1, device_id=peer, device_id_type=MESH)

    def load(src, dst, sem):
        copy = pltpu.make_async_copy(src, dst, sem)
        copy.start()
        return copy

    tokens_load = load(tokens_ref, tokens, load_sem.at[0])
    gain_load = load(gain_in, gains.at[dp], load_sem.at[7])
    small_loads = [load(decay_in, decay_ref, load_sem.at[8]), load(group_in, group_ref, load_sem.at[9])]
    projections = (w0, w1, w2, w3, w4, w5)
    first_loads = [
        load(w.at[0], first_weights.at[pl.ds(n * HEAD, HEAD)], load_sem.at[n + 1]) for n, w in enumerate(projections)
    ]
    wout_loads = [load(out_proj_ref.at[b], wout.at[b, dp], late_sem.at[7 + b]) for b in range(LAYERS)]
    state_load = load(state_ref, state, late_sem.at[0])
    weight_loads = [
        load(w.at[1], weights.at[dp, pl.ds(n * HEAD, HEAD)], late_sem.at[n + 1]) for n, w in enumerate(projections)
    ]

    barrier = pltpu.get_barrier_semaphore()
    tell(barrier, dp_peers + beside(1))

    lane = iota((ROWS, LANES), 1)
    row = iota((ROWS, LANES), 0)
    low_half = lane < HEAD
    eye = (lane == row).astype(jnp.float32)
    pick = (lane % HEAD) // 2 == row
    pick_own = lane % HEAD == 2 * row + lane // HEAD
    ones = jnp.full((2 * LANES, LANES), 1.0, jnp.bfloat16)
    k_of = iota((2 * LANES, LANES), 0)
    l_of = iota((2 * LANES, LANES), 1)
    by_parity = ((k_of // HEAD) % 2 == l_of % 2).astype(jnp.float32).astype(jnp.bfloat16)
    by_half = ((k_of // HEAD) % 2 == l_of // HEAD).astype(jnp.float32).astype(jnp.bfloat16)

    waits = []

    def first_parts():
        columns = [tokens[:, c * LANES : (c + 1) * LANES].astype(jnp.float32) for c in range(4)]
        gain_load.wait()
        normed = jnp.concatenate(
            [(c * gains[dp, 0:1, n * LANES : (n + 1) * LANES]).astype(jnp.bfloat16) for n, c in enumerate(columns)],
            axis=1,
        )
        for copy in first_loads:
            copy.wait()
        part = contract(normed, first_weights[...]).astype(jnp.bfloat16)
        for o in range(8):
            part_send[o] = part[o * ROWS : (o + 1) * ROWS]

    def send_parts():
        for chip in range(4):
            remote(part_send.at[chip * 2 + 1 - core], part_core.at[chip], (pair_sem.at[0], pair_sem.at[1]), (tp, partner))
        waits.append((part_core, pair_sem.at[0]))

    def send_squares():
        columns = [tokens[:, c * LANES : (c + 1) * LANES].astype(jnp.float32) for c in range(4)]
        squares = columns[0] * columns[0]
        for c in columns[1:]:
            squares = squares + c * c
        totals = dot(two_terms(squares), ones)
        for o in range(8):
            sq_send[o] = jnp.sum(totals[o * ROWS : (o + 1) * ROWS] * eye, axis=0, keepdims=True)
        for i, peer in enumerate(dp_peers):
            remote(sq_send.at[peer[1]], sq_recv.at[i], (sq_sem.at[0], sq_sem.at[1]), peer)
        waits.append((sq_recv, sq_sem.at[0]))

    def send_pair_sums():
        wait_for(part_core, pair_sem.at[1])
        for chip in range(4):
            both = part_send[chip * 2 + core].astype(jnp.float32) + part_core[chip].astype(jnp.float32)
            part_sum[chip] = both.astype(jnp.bfloat16)
        for i, o in enumerate((2, 1, 3)):
            chip = lax.rem(x + o, 4)
            remote(part_sum.at[chip], part_recv.at[i], (part_sem.at[0], part_sem.at[1]), (tp, chip * 2 + core))
        waits.append((part_recv, part_sem.at[0]))

    def first_projected():
        wait_for(sq_recv, sq_sem.at[1])
        square = sq_send[dp]
        for i in range(7):
            square = square + sq_recv[i]
        inv = lax.rsqrt(jnp.sum(square * eye, axis=1, keepdims=True) / D + norm_floor)
        wait_for(part_recv, part_sem.at[1])
        total = part_sum[x].astype(jnp.float32)
        for i in range(3):
            total = total + part_recv[i].astype(jnp.float32)
        return total * inv

    def second_projected():
        squares = jnp.zeros((ROWS, LANES), jnp.float32)
        total = jnp.zeros((6 * HEAD, ROWS), jnp.float32)
        held = jnp.zeros((ROWS, 6 * HEAD), jnp.float32)
        arrivals = ((4, 3, 5, 2), (6, 1, 7, 0))
        for a in arrivals[0] + arrivals[1]:
            d = lax.rem(z + 8 - a, 8)
            for group in arrivals:
                if a == group[0]:
                    for other in group:
                        wait_for(x_all.at[pl.ds(0, 8 if other else 7)], x_sem.at[other])
            pieces = []
            for c in range(4):
                at = (d * 4 + c) * 2
                piece = jnp.concatenate([x_all[at], x_all[at + 1]], axis=0).astype(jnp.float32)
                squares = squares + piece * piece
                pieces.append((piece * gains[d, 1:2, c * LANES : (c + 1) * LANES]).astype(jnp.bfloat16))
            total = total + contract(weights[d, :, 0 : 2 * LANES], jnp.concatenate(pieces[:2], axis=1))
            held = held + contract(jnp.concatenate(pieces[2:], axis=1), weights[d, :, 2 * LANES :])
        inv = lax.rsqrt(jnp.sum(squares, axis=1, keepdims=True) / D + norm_floor)
        return (total.T + held) * inv

    def mix(b, projected):
        heads = projected.astype(jnp.bfloat16).astype(jnp.float32)
        both = []
        for n in range(3):
            tile = heads[:, n * LANES : (n + 1) * LANES]
            turned = pltpu.roll(tile, HEAD, 1)
            both.append(jnp.where(low_half, tile, turned))
            both.append(jnp.where(low_half, turned, tile))
        recept, keys, values, decay_part, rate_part, gate_part = both
        base = decay_ref[b : b + 1, :]
        decay = jnp.concatenate([base, base], axis=1) + decay_part
        forget = jnp.exp(-jnp.exp(-jax.nn.softplus(-decay) - 0.5))
        learn = jax.nn.sigmoid(rate_part)
        norm = lax.rsqrt(0.5 * jnp.sum(keys * keys, axis=1, keepdims=True) + 1.0)
        scaled = keys * learn
        with_scaled = 0.5 * jnp.sum(scaled * recept, axis=1, keepdims=True)
        unit = keys * norm
        vec_g[...] = forget * recept - (with_scaled * norm) * unit
        vec_f[...] = forget
        vec_s[...] = scaled
        vec_u[...] = unit * norm
        vec_v[...] = values
        for c in range(4):
            terms = jnp.concatenate([state[b, r] * vec_g[r : r + 1, :] for r in range(c * 8, c * 8 + 8)], axis=0)
            sums = dot(two_terms(terms), by_parity)
            for r in range(8):
                at = c * 8 + r
                chosen = jnp.where(pick, sums[r * ROWS : (r + 1) * ROWS], 0.0)
                read_rows[at : at + 1, :] = jnp.sum(chosen, axis=0, keepdims=True)
        read = read_rows[...] + values * with_scaled
        centre = read - jnp.mean(read, axis=1, keepdims=True)
        normal = centre * lax.rsqrt(jnp.mean(centre * centre, axis=1, keepdims=True) + group_floor)
        gain = group_ref[b : b + 1, :]
        return (normal * jnp.concatenate([gain, gain], axis=1) * jax.nn.sigmoid(gate_part)).astype(jnp.bfloat16)

    own_columns = [lax.rem(x + o, 4) * 2 + core for o in (2, 1, 3, 0)]
    other_columns = [lax.rem(x + o, 4) * 2 + (1 - core) for o in (2, 1, 3, 0)]

    def project_out(b, rows, blocks):
        for d in blocks:
            term = dot(rows, wout[b, d]).astype(jnp.bfloat16)
            for c in range(4):
                for half in range(2):
                    out_send[b, d * 8 + c * 2 + half] = term[
                        half * 16 : (half + 1) * 16, c * LANES : (c + 1) * LANES
                    ]

    def send_out(b):
        for peer in tp_peers:
            remote(out_send.at[b, peer[0]], out_recv.at[b, tp], (out_sem.at[b], out_sem.at[2 + b]), peer)

    def update_state(b):
        for c in range(4):
            terms = jnp.concatenate(
                [
                    jnp.where(pick_own, vec_v[r : r + 1, :], 0.0) - state[b, r] * vec_u[r : r + 1, :]
                    for r in range(c * 8, c * 8 + 8)
                ],
                axis=0,
            )
            sums = dot(two_terms(terms), by_half)
            for r in range(8):
                at = c * 8 + r
                new_state_ref[b, at] = (
                    state[b, at] * vec_f[at : at + 1, :] + sums[r * ROWS : (r + 1) * ROWS] * vec_s[at : at + 1, :]
                )

    def finish_share(b, mine):
        wait_for(out_recv.at[b, pl.ds(0, 63)], out_sem.at[2 + b])
        waits.append((out_recv.at[b, pl.ds(0, 63)], out_sem.at[b]))
        out_recv[b, tp] = out_send[b, tp]
        parts = [out_recv[b, i].astype(jnp.float32) for i in range(4)]
        for i in range(4, 64):
            parts[i % 4] = parts[i % 4] + out_recv[b, i].astype(jnp.float32)
        total = (parts[0] + parts[1]) + (parts[2] + parts[3])
        share[b] = (mine.astype(jnp.float32) + total).astype(jnp.bfloat16)

    def to_partner(b, owner):
        there = wout.at[b, owner]
        remote(there, there, (wout_core_sem.at[b], wout_core_sem.at[2 + b]), (tp, partner))

    def gather_first_wout():
        mine = out_proj_ref.at[0]
        for peer in (far, right, left):
            remote(mine, wout.at[0, dp], (wout_sem.at[0], wout_sem.at[1]), (tp, peer))
        remote(mine, wout.at[0, dp], (wout_core_sem.at[0], wout_core_sem.at[2]), (tp, partner))
        waits.append((wout.at[0, pl.ds(0, 3)], wout_sem.at[0]))

    def pass_first_wout():
        wait_for(wout.at[0, pl.ds(0, 3)], wout_sem.at[1])
        for peer in (far, right, left):
            to_partner(0, peer)
        waits.append((wout.at[0, pl.ds(0, 4)], wout_core_sem.at[0]))

    def gather_second_wout():
        mine = out_proj_ref.at[1]
        remote(mine, wout.at[1, dp], (wout_sem.at[2], wout_sem.at[3]), (tp, left))
        remote(mine, wout.at[1, dp], (wout_sem.at[4], wout_sem.at[5]), (tp, right))
        remote(mine, wout.at[1, dp], (wout_core_sem.at[1], wout_core_sem.at[3]), (tp, partner))
        waits.append((wout.at[1, 0], wout_sem.at[2]))
        waits.append((wout.at[1, 0], wout_sem.at[4]))

    def pass_second_wout():
        from_right = wout.at[1, right]
        wait_for(from_right, wout_sem.at[3])
        remote(from_right, from_right, (wout_sem.at[6], wout_sem.at[7]), (tp, left))
        to_partner(1, right)
        wait_for(wout.at[1, left], wout_sem.at[5])
        to_partner(1, left)
        waits.append((wout.at[1, 0], wout_sem.at[6]))

    def end_second_wout():
        wait_for(wout.at[1, far], wout_sem.at[7])
        to_partner(1, far)
        waits.append((wout.at[1, pl.ds(0, 4)], wout_core_sem.at[1]))

    halves = (pl.ds(0, 192), pl.ds(192, 192))

    def half(owner, n):
        return weights.at[owner, halves[n]]

    def ring_send(owner, n, at, peer):
        there = half(owner, n)
        remote(there, there, (ring_sem.at[at], ring_sem.at[6 + at]), (tp, peer))
        waits.append((half(0, n), ring_sem.at[at]))

    def core_send(owner):
        there = weights.at[owner]
        remote(there, there, (core_sem.at[0], core_sem.at[1]), (tp, partner))

    def gather_weights():
        for copy in weight_loads:
            copy.wait()
        ring_send(dp, 0, 0, right)
        ring_send(dp, 1, 2, left)
        ring_send(dp, 1, 1, right)
        ring_send(dp, 0, 3, left)
        core_send(dp)

    def pass_weights():
        wait_for(half(right, 1), ring_sem.at[8])
        ring_send(right, 1, 5, left)
        wait_for(half(left, 0), ring_sem.at[6])
        ring_send(left, 0, 4, right)

    def pass_to_partner():
        wait_for(half(right, 0), ring_sem.at[9])
        core_send(right)
        wait_for(half(left, 1), ring_sem.at[7])
        core_send(left)

    def end_weights():
        wait_for(half(far, 0), ring_sem.at[10])
        wait_for(half(far, 1), ring_sem.at[11])
        core_send(far)
        waits.append((weights.at[pl.ds(0, 4)], core_sem.at[0]))

    pl.semaphore_wait(barrier, 11)
    gather_first_wout()
    tell(near_sem, beside(1))
    tokens_load.wait()
    first_parts()
    send_parts()
    send_squares()
    send_pair_sums()
    for peer in dp_peers:
        remote(gains.at[dp], gains.at[dp], (gain_sem.at[0], gain_sem.at[1]), peer)
    waits.append((gains.at[pl.ds(0, 7)], gain_sem.at[0]))
    at_column = pl.ds(pl.multiple_of(column * LANES, LANES), LANES)

    def at_rows(owner):
        return pl.ds(pl.multiple_of(owner * ROWS + half_row * 16, 16), 16)

    @pl.when(owns_columns)
    def _():
        for peer in dp_peers:
            remote(tokens.at[at_rows(peer[1]), at_column], residue, (residue_sem.at[0], residue_sem.at[1]), peer)
        residue[...] = tokens[at_rows(dp), at_column]

    pl.semaphore_wait(near_sem, 4)
    tell(line_sem, beside(2))
    pl.semaphore_wait(line_sem, 4)
    tell(row_sem, z_peers)
    gather_weights()
    gather_second_wout()
    pass_first_wout()
    projected = first_projected()
    for copy in small_loads + [state_load]:
        copy.wait()
    mixed = mix(0, projected)[:, :HEAD]
    pl.semaphore_wait(row_sem, 7)
    tell(plane_sem, dp_peers)
    for copy in wout_loads:
        copy.wait()
    project_out(0, mixed, own_columns)
    wait_for(wout.at[0, pl.ds(0, 4)], wout_core_sem.at[2])
    project_out(0, mixed, other_columns)
    send_out(0)
    update_state(0)
    pass_weights()
    pass_to_partner()

    @pl.when(jnp.logical_not(owns_columns))
    def _():
        wait_for(residue, residue_sem.at[1])

    finish_share(0, residue[...])
    x_all[tp] = share[0]
    for peer, (a, _) in zip(tp_peers, TP_OFFSETS):
        remote(share.at[0], x_all.at[tp], (x_sem.at[8], x_sem.at[a]), peer)
    waits.append((x_all.at[pl.ds(0, 63)], x_sem.at[8]))
    pass_second_wout()
    end_weights()
    end_second_wout()
    wait_for(gains.at[pl.ds(0, 7)], gain_sem.at[1])
    pl.semaphore_wait(plane_sem, 7)
    wait_for(weights.at[pl.ds(0, 4)], core_sem.at[1])

    mixed = mix(1, second_projected())[:, :HEAD]
    wait_for(wout.at[1, pl.ds(0, 4)], wout_core_sem.at[3])
    project_out(1, mixed, range(8))
    send_out(1)
    update_state(1)
    finish_share(1, share[0])
    slot = (dp * 2 + half_row) * 4 + column

    @pl.when(jnp.logical_not(owns_columns))
    def _():
        remote(share.at[1], x_last.at[slot], (last_sem.at[2], last_sem.at[1]), (tp, z))

    @pl.when(owns_columns)
    def _():
        load(share.at[1], x_last.at[slot], last_sem.at[1])

    for peer in tp_peers:
        remote(share.at[1], x_last.at[slot], (last_sem.at[0], last_sem.at[1]), (peer[0], z))
    waits.append((x_last.at[pl.ds(0, 63)], last_sem.at[0]))
    wait_for(x_last, last_sem.at[1])
    for g in range(16):
        for c in range(4):
            next_ref[g * 16 : (g + 1) * 16, c * LANES : (c + 1) * LANES] = x_last[g * 4 + c]

    @pl.when(jnp.logical_not(owns_columns))
    def _():
        wait_for(share.at[1], last_sem.at[2])

    @pl.when(owns_columns)
    def _():
        wait_for(x_last.at[pl.ds(0, 7)], residue_sem.at[0])

    for ref, sem in waits:
        wait_for(ref, sem)


def write_out(next_ref, state_ref, next_out, state_out, sems):
    copies = [
        pltpu.make_async_copy(src, dst, sems.at[n])
        for n, (src, dst) in enumerate(((state_ref, state_out), (next_ref, next_out)))
    ]
    for copy in copies:
        copy.start()
    for copy in copies:
        copy.wait()


def shards(
    tokens,
    norm_gain,
    receptance,
    key_proj,
    value_proj,
    decay_proj,
    rate_proj,
    gate_proj,
    decay_base,
    group_gain,
    output_proj,
    state,
):
    flat = [jnp.swapaxes(w, 1, 2) for w in (receptance, key_proj, value_proj, decay_proj, rate_proj, gate_proj)]
    remote = pl.BlockSpec(memory_space=pltpu.HBM)
    local = pl.BlockSpec(memory_space=pltpu.VMEM)
    f32, bf16 = jnp.float32, jnp.bfloat16
    dma = pltpu.SemaphoreType.DMA

    current, updated = pl.pallas_call(
        body,
        out_shape=(
            pltpu.VMEM((256, WIDE), bf16),
            pltpu.VMEM((LAYERS, ROWS, 32, LANES), f32),
        ),
        in_specs=[remote] * 12,
        out_specs=(local, local),
        scratch_shapes=[
            pltpu.VMEM((256, WIDE), bf16),
            pltpu.VMEM((6 * HEAD, WIDE), bf16),
            pltpu.VMEM((8, 6 * HEAD, WIDE), bf16),
            pltpu.VMEM((LAYERS, 8, HEAD, WIDE), bf16),
            pltpu.VMEM((8, LAYERS, WIDE), f32),
            pltpu.VMEM((LAYERS, HEAD), f32),
            pltpu.VMEM((LAYERS, HEAD), f32),
            pltpu.VMEM((16, LANES), bf16),
            pltpu.VMEM((LAYERS, ROWS, 32, LANES), f32),
            pltpu.VMEM((8, ROWS, 6 * HEAD), bf16),
            pltpu.VMEM((4, ROWS, 6 * HEAD), bf16),
            pltpu.VMEM((4, ROWS, 6 * HEAD), bf16),
            pltpu.VMEM((3, ROWS, 6 * HEAD), bf16),
            pltpu.VMEM((8, 1, LANES), f32),
            pltpu.VMEM((7, 1, LANES), f32),
            pltpu.VMEM((LAYERS, 64, 16, LANES), bf16),
            pltpu.VMEM((LAYERS, 64, 16, LANES), bf16),
            pltpu.VMEM((LAYERS, 16, LANES), bf16),
            pltpu.VMEM((64, 16, LANES), bf16),
            pltpu.VMEM((64, 16, LANES), bf16),
        ]
        + [pltpu.VMEM((ROWS, LANES), f32)] * 6
        + [dma((10,)), dma((9,)), dma((2,)), dma((2,)), dma((2,)), dma((4,)), dma((9,)), dma((2,)), dma((2,))]
        + [dma((8,)), dma((4,)), dma((12,)), dma((2,)), dma((3,))]
        + [pltpu.SemaphoreType.REGULAR] * 4,
        compiler_params=pltpu.CompilerParams(
            collective_id=0, has_side_effects=True, vmem_limit_bytes=32 * 1024 * 1024
        ),
        name="blocks",
    )(
        *[
            pltpu.with_memory_space_constraint(a, pltpu.HBM)
            for a in (
                tokens,
                norm_gain,
                *flat,
                decay_base,
                group_gain,
                output_proj,
                state.reshape(LAYERS, ROWS, 32, LANES),
            )
        ]
    )
    current, updated = pl.pallas_call(
        write_out,
        out_shape=(
            jax.ShapeDtypeStruct((256, WIDE), bf16),
            jax.ShapeDtypeStruct((LAYERS, ROWS, 32, LANES), f32),
        ),
        in_specs=[local, local],
        out_specs=(remote, remote),
        scratch_shapes=[dma((2,))],
        name="write_out",
    )(*[pltpu.with_memory_space_constraint(a, pltpu.VMEM) for a in (current, updated)])
    return (current, updated.reshape(LAYERS, ROWS, 1, HEAD * HEAD))


def solution(mesh):
    return jax.shard_map(
        shards,
        mesh=mesh,
        in_specs=(
            P(None, "dp"),
            P(None, "dp"),
            P(None, "dp", "tp"),
            P(None, "dp", "tp"),
            P(None, "dp", "tp"),
            P(None, "dp", "tp"),
            P(None, "dp", "tp"),
            P(None, "dp", "tp"),
            P(None, "tp"),
            P(None, "tp"),
            P(None, "tp", "dp"),
            P(None, "dp", "tp", None),
        ),
        out_specs=(P(None, "dp"), P(None, "dp", "tp", None)),
        check_vma=False,
    )
```
